32 devices in a mesh: ep: 8 (over z, core), tp: 4 (over y, x).
Axes of the slice: x: 2, y: 2, z: 4, core: 2. Of those that a mesh axis runs over, the one named last changes fastest.
Arguments:
- tokens: bfloat16 [384, 2048], P('ep', 'tp'), may hold values from -64 to 64
- mix_gain: float32 [2048], replicated, may hold values from 0.1 to 1.9
- w_gate_z: bfloat16 [2048, 2048], P(None, 'tp'), may hold values from -0.125 to 0.125
- w_value_x: bfloat16 [2048, 2048], P(None, 'tp'), may hold values from -0.125 to 0.125
- w_key_b: bfloat16 [2048, 256], replicated, may hold values from -0.125 to 0.125
- w_query_c: bfloat16 [2048, 256], replicated, may hold values from -0.125 to 0.125
- w_step: bfloat16 [2048, 32], replicated, may hold values from -0.125 to 0.125
- step_bias: float32 [32], replicated, may hold values from -2 to 1
- decay_log: float32 [32], replicated, may hold values from -3 to 1.4
- skip_gain: float32 [32], replicated, may hold values from 0.1 to 1.9
- conv_x_weight: bfloat16 [4, 2048], P(None, 'tp'), may hold values from -3 to 3
- conv_b_weight: bfloat16 [4, 256], replicated, may hold values from -3 to 3
- conv_c_weight: bfloat16 [4, 256], replicated, may hold values from -3 to 3
- window_x: bfloat16 [384, 3, 2048], P('ep', None, 'tp'), may hold values from -6 to 6
- window_b: bfloat16 [384, 3, 256], P('ep'), may hold values from -6 to 6
- window_c: bfloat16 [384, 3, 256], P('ep'), may hold values from -6 to 6
- ssm_state: float32 [384, 32, 64, 128], P('ep', 'tp'), may hold values from -2 to 2
- head_gain: float32 [2048], P('tp'), may hold values from 0.1 to 1.9
- w_out: bfloat16 [2048, 2048], P('tp'), may hold values from -0.1875 to 0.1875
- ffn_gain: float32 [2048], replicated, may hold values from 0.1 to 1.9
- route_ids: int32 [384, 2], P('ep'), may hold values from 0 to 31, all different within a row; in each aligned block of 48 rows (0 to 47, 48 to 95, ...) at most 5 rows name the same one
- route_weights: float32 [384, 2], P('ep'), may hold values from 0.05 to 1
- expert_gate: bfloat16 [8, 2048, 4096], P('ep', None, 'tp'), may hold values from -0.125 to 0.125
- expert_up: bfloat16 [8, 2048, 4096], P('ep', None, 'tp'), may hold values from -0.125 to 0.125
- expert_down: bfloat16 [8, 4096, 2048], P('ep', 'tp'), may hold values from -0.25 to 0.25
Outputs:
- layer_out: bfloat16 [384, 2048], P('ep', 'tp')
The draws below stay inside these ranges and needn't reach their ends.
Inputs may be any that keep to these rules, and one draw needn't show every extreme that they name: `route_ids`: each row names 2 different experts. Within the rows of one index of ep (aligned blocks of 48 rows) no expert is named by more than 5 rows, a bound that some block reaches.
All inputs are finite; a program needn't handle non-finite values.
Results may differ from the reference program's by a relative error of at most 0.009.
Values may be sent and summed in bfloat16 or wider, within the bound.
No kernel may reach another device: no remote copies, remote signals or barrier semaphores. Data moves between devices by JAX's collectives and lax.ppermute only.
A program may use at most 64 MiB of HBM per device.

```python
import math
import jax
import jax.numpy as jnp
import numpy as np
from jax import lax

D = 2048
HEADS = 32
HEAD_DIM = 64
STATE = 128
GROUPS = 2
CONV = 4
FE = 1024
EXP_IN = 4
TOPK = 2
SEQ_DEV = 48
SSD_W = 2048
GN = 256
SEQS = 384
SETS = 8
EXPERTS = 32
SET_UNITS = 4096
CAP = 5
N_EP = 8


def draw_tokens(key, part):
    base_key = jax.random.fold_in(key, 11)
    row_key, column_key, body_key = jax.random.split(base_key, 3)
    row_scale = jnp.exp(jax.random.uniform(row_key, (SEQS, 1), jnp.float32, math.log(0.3), math.log(3.0)))
    column_scale = jnp.exp(jax.random.uniform(column_key, (1, D), jnp.float32, math.log(0.3), math.log(3.0)))
    pattern = jax.random.normal(body_key, (SEQS, D), jnp.float32)
    pattern = jnp.clip(pattern, -6.0, 6.0)
    return (pattern * row_scale * column_scale).astype(jnp.bfloat16)


def raised(entries, stream_key, source, target, shards_of, factor):
    owner, partner = [(jnp.arange(entries.shape[axis_at]) // (entries.shape[axis_at] // shards_of)).reshape([-1 if axis == axis_at else 1 for axis in range(entries.ndim)]) for axis_at in (source, target)]
    chosen = jax.random.permutation(stream_key, shards_of)[partner]
    strong = (owner == chosen) | (owner == (partner + shards_of // 2) % shards_of)
    return jnp.where(strong, factor * entries, entries)


def steps_of(rng, dims, shards, low, top_value):
    factor_of = 1.0
    for axis_at, parts in shards:
        heights = jax.random.uniform(jax.random.fold_in(jax.random.fold_in(rng, 6), axis_at), (parts,), jnp.float32, low / len(shards), top_value / len(shards))
        factor_of = factor_of * jnp.repeat(jnp.exp(heights), dims[axis_at] // parts).reshape((-1,) + (1,) * (len(dims) - 1 - axis_at))
    return factor_of


def deal_out(stream_key, own, number, rows, number_of, top, bound, slope):
    ranking = jax.random.permutation(stream_key, number_of)
    crowded, usual = load_shares(number_of, rows * top, bound, slope, True), load_shares(number_of, rows * top, bound, slope, False)
    places = jnp.arange(number_of)

    def named(lengths, offset_by):
        used = int((lengths > 0).sum())
        fixed = max(1, used // 4)
        moved = fixed + (places - fixed + offset_by * (used - fixed)) % max(1, number_of - fixed)
        return jnp.zeros((number_of,), jnp.int32).at[ranking[jnp.where(places < fixed, places, moved)]].set(jnp.asarray(lengths, jnp.int32))

    lengths = jnp.where(number % 4 == 0, named(crowded, number // 4), named(usual, number - number // 4 - 1))
    mixed = jax.random.permutation(jax.random.fold_in(own, 3), number_of)
    source_of, taker = mixed[0:number_of // 2 * 2:2], mixed[1:number_of // 2 * 2:2]
    margin = jnp.minimum(lengths[source_of] - 1, bound - lengths[taker]) // 2
    margin = jnp.where((source_of == ranking[0]) | (taker == ranking[0]) | (lengths[taker] == 0), 0, jnp.maximum(margin, 0))
    moved = jax.random.randint(jax.random.fold_in(own, 4), (number_of // 2,), 0, 1 << 20) % (margin + 1)
    lengths = lengths.at[source_of].add(-moved).at[taker].add(moved)
    labels = jnp.searchsorted(jnp.cumsum(lengths), jnp.arange(rows * top), side="right").astype(jnp.int32)
    table = labels.reshape(top, rows).T
    table = table[jax.random.permutation(jax.random.fold_in(own, 1), rows)]
    offset_by = jax.random.randint(jax.random.fold_in(own, 2), (rows, 1), 0, top)
    return jnp.take_along_axis(table, (jnp.arange(top)[None, :] + offset_by) % top, axis=1)


def load_shares(amount, total, reach, lean, full):
    portions = [(1 << 20) // math.isqrt(rank ** lean) + 1 for rank in range(1, amount + 1)]
    largest = reach if full else min(reach, max(-(-total // amount), total * portions[0] // sum(portions)))
    least = 1 if total - largest >= amount - 1 else 0
    given, rest = [largest] + [least] * (amount - 1), total - largest - least * (amount - 1)
    while rest > 0:
        free = [i for i in range(1, amount) if given[i] < largest] or [i for i in range(1, amount) if given[i] < reach]
        mass, left = sum([portions[i] for i in free]), rest
        for i in free:
            addition = min(reach - given[i], max(1, left * portions[i] // mass), rest)
            given[i] = given[i] + addition
            rest = rest - addition
    return np.array(given)


def noise(own_key, dims, width, limit, shards=(), kind=jnp.bfloat16):
    array = jax.random.normal(own_key, dims, jnp.float32) * width
    if len(shards) > 0:
        array = steps_of(own_key, dims, shards, -0.22, 0.18) * array
    return jnp.clip(array, min=-limit, max=limit).astype(kind)


def heavy_noise(stream_key, extent, spread, reach, pieces, heavy, held_as=jnp.bfloat16):
    entries = spread * jax.random.normal(stream_key, extent, jnp.float32)
    if pieces:
        entries = entries * steps_of(stream_key, extent, pieces, -0.22, 0.18)
    return jnp.clip(raised(entries, jax.random.fold_in(stream_key, 3), *heavy), -reach, reach).astype(held_as)


def setup_inputs(seed: int = 0) -> dict:
    arg_keys = jax.random.split(jax.random.key(seed), 26)
    tokens = draw_tokens(jax.random.fold_in(arg_keys[25], 71), 0)
    mix_gain = jnp.clip(1.0 + 0.18 * jax.random.normal(arg_keys[1], (D,), jnp.float32), 0.1, 1.9)
    w_gate_z = noise(arg_keys[2], (D, SSD_W), D ** -0.5, 0.125, ((1, 4),))
    w_value_x = noise(arg_keys[3], (D, SSD_W), D ** -0.5, 0.125, ((1, 4),))
    w_key_b = noise(arg_keys[4], (D, GN), D ** -0.5, 0.125)
    w_query_c = noise(arg_keys[5], (D, GN), D ** -0.5, 0.125)
    w_step = noise(arg_keys[6], (D, HEADS), D ** -0.5, 0.125)
    step_bias = jnp.clip(jax.random.uniform(arg_keys[7], (HEADS,), jnp.float32, -2.0, 1.0), -2.0, 1.0)
    decay_log = jnp.clip(jax.random.uniform(arg_keys[8], (HEADS,), jnp.float32, -3.0, 1.4), -3.0, 1.4)
    skip_gain = jnp.clip(1.0 + 0.18 * jax.random.normal(arg_keys[9], (HEADS,), jnp.float32), 0.1, 1.9)
    conv_x_weight = noise(arg_keys[10], (CONV, SSD_W), CONV ** -0.5, 3.0, ((1, 4),))
    conv_b_weight = noise(arg_keys[11], (CONV, GN), CONV ** -0.5, 3.0)
    conv_c_weight = noise(arg_keys[12], (CONV, GN), CONV ** -0.5, 3.0)
    window_x = noise(arg_keys[13], (SEQS, CONV - 1, SSD_W), 1.0, 6.0, ((0, 8), (2, 4)))
    window_b = noise(arg_keys[14], (SEQS, CONV - 1, GN), 1.0, 6.0, ((0, 8),))
    window_c = noise(arg_keys[15], (SEQS, CONV - 1, GN), 1.0, 6.0, ((0, 8),))
    ssm_state = noise(arg_keys[16], (SEQS, HEADS, HEAD_DIM, STATE), 0.3, 2.0, ((0, 8), (1, 4)), jnp.float32)
    head_gain = jnp.clip(1.0 + 0.18 * jax.random.normal(arg_keys[17], (SSD_W,), jnp.float32), 0.1, 1.9)
    w_out = heavy_noise(arg_keys[18], (SSD_W, D), SSD_W ** -0.5, 0.1875, ((0, 4),), (0, 1, 4, 2.0))
    ffn_gain = jnp.clip(1.0 + 0.18 * jax.random.normal(arg_keys[19], (D,), jnp.float32), 0.1, 1.9)
    route_ids_keys = jax.random.split(jax.random.fold_in(arg_keys[20], 1), SEQS // SEQ_DEV)
    route_ids_turns = jax.random.permutation(jax.random.fold_in(arg_keys[20], 3), SEQS // SEQ_DEV)
    route_ids = jax.vmap(lambda own, number: deal_out(jax.random.fold_in(arg_keys[20], 2), own, number, SEQ_DEV, EXPERTS, TOPK, CAP, 2))(route_ids_keys, route_ids_turns).reshape((SEQS, TOPK))
    route_weights = jnp.clip(0.05 + 0.95 * jax.random.uniform(arg_keys[21], (SEQS, TOPK), jnp.float32) ** steps_of(arg_keys[21], (SEQS, TOPK), ((0, 8),), -0.2, 0.2), 0.05, 1.0)
    expert_gate = noise(arg_keys[22], (SETS, D, SET_UNITS), D ** -0.5, 0.125, ((0, 8), (2, 4)))
    expert_up = noise(arg_keys[23], (SETS, D, SET_UNITS), D ** -0.5, 0.125, ((0, 8), (2, 4)))
    expert_down = heavy_noise(arg_keys[24], (SETS, SET_UNITS, D), FE ** -0.5, 0.25, ((0, 8), (1, 4)), (1, 2, 4, 2.0))
    return {"tokens": tokens, "mix_gain": mix_gain, "w_gate_z": w_gate_z, "w_value_x": w_value_x, "w_key_b": w_key_b, "w_query_c": w_query_c, "w_step": w_step, "step_bias": step_bias, "decay_log": decay_log, "skip_gain": skip_gain, "conv_x_weight": conv_x_weight, "conv_b_weight": conv_b_weight, "conv_c_weight": conv_c_weight, "window_x": window_x, "window_b": window_b, "window_c": window_c, "ssm_state": ssm_state, "head_gain": head_gain, "w_out": w_out, "ffn_gain": ffn_gain, "route_ids": route_ids, "route_weights": route_weights, "expert_gate": expert_gate, "expert_up": expert_up, "expert_down": expert_down}


norm_epsilon = 1e-06

def row_norm(arr_values, norm_gain):
    widened = arr_values.astype(jnp.float32)
    return widened * lax.rsqrt(lax.optimization_barrier(jnp.mean(widened * widened, axis=-1, keepdims=True)) + norm_epsilon) * norm_gain

def short_conv(window, fresh_row, weight):
    conv_taps = weight.astype(jnp.float32)
    summed = lax.optimization_barrier(jnp.sum(window.astype(jnp.float32) * conv_taps[:-1][None], axis=1)) + fresh_row * conv_taps[-1]
    return jax.nn.silu(summed)

def product(left, right):
    return jnp.dot(left, right, preferred_element_type=jnp.float32)

def reference(tokens, mix_gain, w_gate_z, w_value_x, w_key_b, w_query_c, w_step, step_bias, decay_log, skip_gain, conv_x_weight, conv_b_weight, conv_c_weight, window_x, window_b, window_c, ssm_state, head_gain, w_out, ffn_gain, route_ids, route_weights, expert_gate, expert_up, expert_down):
    seq_count = tokens.shape[0]
    normed = row_norm(tokens, mix_gain).astype(jnp.bfloat16)
    gate_z = product(normed, w_gate_z)
    values = short_conv(window_x, product(normed, w_value_x), conv_x_weight)
    keys = short_conv(window_b, product(normed, w_key_b), conv_b_weight)
    queries = short_conv(window_c, product(normed, w_query_c), conv_c_weight)
    step_size = jax.nn.softplus(product(normed, w_step) + step_bias)
    decay_heads = jnp.exp(-step_size * jnp.exp(decay_log))
    per_group = HEADS // GROUPS
    value_heads = values.reshape(seq_count, HEADS, HEAD_DIM)
    key_heads = jnp.repeat(keys.reshape(seq_count, GROUPS, STATE), per_group, axis=1)
    query_heads = jnp.repeat(queries.reshape(seq_count, GROUPS, STATE), per_group, axis=1)
    new_state = decay_heads[:, :, None, None] * ssm_state + (step_size[:, :, None] * value_heads)[..., None] * key_heads[:, :, None, :]
    read_out = jnp.einsum('shpn,shn->shp', new_state, query_heads, precision=lax.Precision.HIGHEST)
    read_out = read_out + skip_gain[None, :, None] * value_heads
    gated = read_out * jax.nn.silu(gate_z.reshape(seq_count, HEADS, HEAD_DIM))
    gated = gated * lax.rsqrt(lax.optimization_barrier(jnp.mean(gated * gated, axis=-1, keepdims=True)) + norm_epsilon)
    mixed_heads = (gated * head_gain.reshape(HEADS, HEAD_DIM)).reshape(seq_count, SSD_W).astype(jnp.bfloat16)
    mix_out = product(mixed_heads, w_out)
    residual = (tokens.astype(jnp.float32) + mix_out).astype(jnp.bfloat16)
    ffn_in = row_norm(residual, ffn_gain).astype(jnp.bfloat16)
    route_share = route_weights / lax.optimization_barrier(jnp.sum(route_weights, axis=1, keepdims=True))
    rows_most = N_EP * CAP
    row_order = jnp.arange(seq_count, dtype=jnp.int32)
    zero_index = jnp.zeros((), jnp.int32)

    def one_expert(running, expert):
        hit_mask = route_ids == expert
        weight = lax.optimization_barrier(jnp.sum(jnp.where(hit_mask, route_share, 0.0), axis=1))
        taken_rows = jnp.any(hit_mask, axis=1)
        rank_key = jnp.where(taken_rows, 0, seq_count).astype(jnp.int32) + row_order
        picked = jnp.argsort(rank_key)[:rows_most].astype(jnp.int32)
        chosen_rows = ffn_in[picked]
        set_index = (expert // EXP_IN).astype(jnp.int32)
        sub_start = (expert % EXP_IN * FE).astype(jnp.int32)
        gate_block = lax.dynamic_slice(expert_gate, (set_index, zero_index, sub_start), (1, D, FE))[0]
        up_block = lax.dynamic_slice(expert_up, (set_index, zero_index, sub_start), (1, D, FE))[0]
        down_block = lax.dynamic_slice(expert_down, (set_index, sub_start, zero_index), (1, FE, D))[0]
        hidden = (jax.nn.silu(product(chosen_rows, gate_block)) * product(chosen_rows, up_block)).astype(jnp.bfloat16)
        result = product(hidden, down_block)
        running = running.at[picked].add(weight[picked][:, None] * result)
        return (running, None)
    moe_sum, unused = lax.scan(one_expert, jnp.zeros((seq_count, D), jnp.float32), jnp.arange(EXPERTS, dtype=jnp.int32))
    return (residual.astype(jnp.float32) + moe_sum).astype(jnp.bfloat16)
```

```python
import jax
import jax.numpy as jnp
from jax import lax
from jax.experimental import pallas as pl
from jax.experimental.pallas import tpu as pltpu
from jax.sharding import PartitionSpec as P

HEADS = 32
HEAD_DIM = 64
STATE = 128
GROUPS = 2
EXP_IN = 4


norm_epsilon = 1e-06


def row_norm(arr_values, norm_gain):
    widened = arr_values.astype(jnp.float32)
    return (
        widened
        * lax.rsqrt(jnp.mean(widened * widened, axis=-1, keepdims=True) + norm_epsilon)
        * norm_gain
    )


def short_conv(window, fresh_row, weight):
    conv_taps = weight.astype(jnp.float32)
    summed = (
        jnp.sum(window.astype(jnp.float32) * conv_taps[:-1][None], axis=1)
        + fresh_row * conv_taps[-1]
    )
    return jax.nn.silu(summed)


def product(left, right):
    return jnp.dot(left, right, preferred_element_type=jnp.float32)


def local_generic(
    tokens,
    mix_gain,
    w_gate_z,
    w_value_x,
    w_key_b,
    w_query_c,
    w_step,
    step_bias,
    decay_log,
    skip_gain,
    conv_x_weight,
    conv_b_weight,
    conv_c_weight,
    window_x,
    window_b,
    window_c,
    ssm_state,
    head_gain,
    w_out,
    ffn_gain,
    route_ids,
    route_weights,
    expert_gate,
    expert_up,
    expert_down,
):
    tp_index = lax.axis_index("tp")
    tp_count = lax.axis_size("tp")
    ep_count = lax.axis_size("ep")
    seq_count = tokens.shape[0]
    gathered = lax.all_gather(tokens, "tp", axis=1, tiled=True)
    normed = row_norm(gathered, mix_gain).astype(jnp.bfloat16)
    local_width = w_gate_z.shape[1]
    head_count = local_width // HEAD_DIM
    first_head = tp_index * head_count
    group_start = first_head // (HEADS // GROUPS) * STATE
    gate_z = product(normed, w_gate_z)
    values = short_conv(window_x, product(normed, w_value_x), conv_x_weight)
    key_b = short_conv(
        lax.dynamic_slice_in_dim(window_b, group_start, STATE, 2),
        product(normed, lax.dynamic_slice_in_dim(w_key_b, group_start, STATE, 1)),
        lax.dynamic_slice_in_dim(conv_b_weight, group_start, STATE, 1),
    )
    query_c = short_conv(
        lax.dynamic_slice_in_dim(window_c, group_start, STATE, 2),
        product(normed, lax.dynamic_slice_in_dim(w_query_c, group_start, STATE, 1)),
        lax.dynamic_slice_in_dim(conv_c_weight, group_start, STATE, 1),
    )
    step_all = product(normed, w_step) + step_bias
    step_size = jax.nn.softplus(lax.dynamic_slice_in_dim(step_all, first_head, head_count, 1))
    rate_heads = jnp.exp(lax.dynamic_slice_in_dim(decay_log, first_head, head_count, 0))
    skip_heads = lax.dynamic_slice_in_dim(skip_gain, first_head, head_count, 0)
    decay_heads = jnp.exp(-step_size * rate_heads)
    value_heads = values.reshape(seq_count, head_count, HEAD_DIM)
    new_state = (
        decay_heads[:, :, None, None] * ssm_state
        + (step_size[:, :, None] * value_heads)[..., None] * key_b[:, None, None, :]
    )
    read_out = jnp.einsum("shpn,sn->shp", new_state, query_c, precision=lax.Precision.HIGHEST)
    read_out = read_out + skip_heads[None, :, None] * value_heads
    gated = read_out * jax.nn.silu(gate_z.reshape(seq_count, head_count, HEAD_DIM))
    gated = gated * lax.rsqrt(jnp.mean(gated * gated, axis=-1, keepdims=True) + norm_epsilon)
    mixed_heads = (
        (gated * head_gain.reshape(head_count, HEAD_DIM))
        .reshape(seq_count, local_width)
        .astype(jnp.bfloat16)
    )
    partial_value = product(mixed_heads, w_out)
    share_mix = lax.psum_scatter(partial_value, "tp", scatter_dimension=1, tiled=True)
    residual_own = (tokens.astype(jnp.float32) + share_mix).astype(jnp.bfloat16)
    residual_full = lax.all_gather(residual_own, "tp", axis=1, tiled=True)
    ffn_in = row_norm(residual_full, ffn_gain).astype(jnp.bfloat16)
    top_count = route_ids.shape[1]
    expert_count = EXP_IN * ep_count
    capacity = max(2, (3 * seq_count * top_count + 2 * expert_count - 1) // (2 * expert_count))
    sub_index = tp_index // (tp_count // EXP_IN)
    target_set = route_ids // EXP_IN
    hit_mask = route_ids % EXP_IN == sub_index
    set_grid = jnp.arange(ep_count, dtype=jnp.int32)
    set_onehot = (hit_mask[:, :, None] & (target_set[:, :, None] == set_grid)).astype(jnp.int32)
    set_onehot = set_onehot.reshape(seq_count * top_count, ep_count)
    earlier = jnp.cumsum(set_onehot, axis=0) - set_onehot
    slot_rank = jnp.sum(earlier * set_onehot, axis=1).reshape(seq_count, top_count)
    slot_index = jnp.where(hit_mask, target_set * capacity + slot_rank, -1)
    slot_grid = jnp.arange(ep_count * capacity, dtype=jnp.int32)
    slot_match = slot_index[:, :, None] == slot_grid
    placed = jnp.any(slot_match, axis=1).astype(jnp.bfloat16)
    outgoing = jnp.einsum("sj,sd->jd", placed, ffn_in, preferred_element_type=jnp.float32)
    outgoing = outgoing.astype(jnp.bfloat16).reshape(ep_count, capacity, ffn_in.shape[1])
    route_share = route_weights / jnp.sum(route_weights, axis=1, keepdims=True)
    combine_weight = jnp.sum(jnp.where(slot_match, route_share[:, :, None], 0.0), axis=1)
    arrived = lax.all_to_all(outgoing, "ep", split_axis=0, concat_axis=0, tiled=True)
    source_count, slot_count, row_width = arrived.shape
    flat_rows = arrived.reshape(source_count * slot_count, row_width)
    gate_part = product(flat_rows, expert_gate[0])
    up_part = product(flat_rows, expert_up[0])
    hidden = (jax.nn.silu(gate_part) * up_part).astype(jnp.bfloat16)
    expert_out = product(hidden, expert_down[0]).reshape(source_count, slot_count, row_width)
    returned = lax.all_to_all(
        expert_out.astype(jnp.bfloat16), "ep", split_axis=0, concat_axis=0, tiled=True
    ).astype(expert_out.dtype)
    moe_part = jnp.dot(
        combine_weight,
        returned.reshape(ep_count * capacity, -1),
        precision=lax.Precision.HIGHEST,
        preferred_element_type=jnp.float32,
    )
    moe_share = lax.psum_scatter(
        moe_part.astype(jnp.bfloat16), "tp", scatter_dimension=1, tiled=True
    ).astype(jnp.float32)
    return (residual_own.astype(jnp.float32) + moe_share).astype(jnp.bfloat16)


ROW_TILE = 8
LANES = 128


def dot_bf16(left, right):
    return lax.dot_general(left, right, (((1,), (0,)), ((), ())), preferred_element_type=jnp.float32)


def dot_nt(left, right, precision=None):
    return lax.dot_general(
        left, right, (((1,), (1,)), ((), ())), precision=precision, preferred_element_type=jnp.float32
    )


def dot_exact(left, right):
    return lax.dot_general(
        left,
        right,
        (((1,), (0,)), ((), ())),
        precision=lax.Precision.HIGHEST,
        preferred_element_type=jnp.float32,
    )


def silu(value):
    return value / (1.0 + jnp.exp(-value))


def conv_rows(window_ref, columns, fresh, taps_ref):
    taps = taps_ref[:, columns].astype(jnp.float32)
    count = window_ref.shape[0]
    summed = fresh * taps[count : count + 1]
    for tap in range(count):
        summed = summed + window_ref[tap, :, columns].astype(jnp.float32) * taps[tap : tap + 1]
    return silu(summed)


def mixer_body(
    row_ref,
    gain_ref,
    step_w_ref,
    bias_ref,
    rate_ref,
    skip_ref,
    tap_x_ref,
    tap_b_ref,
    tap_c_ref,
    win_x_ref,
    win_b_ref,
    win_c_ref,
    head_gain_ref,
    gate_hbm,
    value_hbm,
    key_hbm,
    query_hbm,
    state_hbm,
    out_w_hbm,
    part_ref,
    gate_w,
    value_w,
    key_w,
    query_w,
    state,
    out_w,
    y_ref,
    w_sems,
    s_sems,
):
    tp_index = lax.axis_index("tp")
    seqs, width = y_ref.shape
    head_count = width // HEAD_DIM
    first_head = tp_index * head_count
    group = first_head // (HEADS // GROUPS)
    columns = pl.ds(pl.multiple_of(group * STATE, STATE), STATE)
    copies = [
        pltpu.make_async_copy(key_hbm.at[:, columns], key_w, w_sems.at[0]),
        pltpu.make_async_copy(query_hbm.at[:, columns], query_w, w_sems.at[1]),
        pltpu.make_async_copy(value_hbm, value_w, w_sems.at[2]),
        pltpu.make_async_copy(gate_hbm, gate_w, w_sems.at[3]),
        pltpu.make_async_copy(out_w_hbm, out_w, w_sems.at[4]),
    ]
    blocks = seqs // ROW_TILE
    state_copies = [
        pltpu.make_async_copy(
            state_hbm.at[pl.ds(b * ROW_TILE, ROW_TILE)], state.at[pl.ds(b * ROW_TILE, ROW_TILE)], s_sems.at[b]
        )
        for b in range(blocks)
    ]
    for copy in copies[:2] + state_copies + copies[2:]:
        copy.start()
    rows = row_ref[...].astype(jnp.float32)
    scale = lax.rsqrt(jnp.mean(rows * rows, axis=-1, keepdims=True) + norm_epsilon)
    normed = (rows * scale * gain_ref[...]).astype(jnp.bfloat16)
    step_size = jax.nn.softplus(dot_nt(normed, step_w_ref[...]) + bias_ref[...])
    decay = jnp.exp(-step_size * jnp.exp(rate_ref[...]))
    copies[0].wait()
    keys = conv_rows(win_b_ref, columns, dot_bf16(normed, key_w[...]), tap_b_ref)
    copies[1].wait()
    queries = conv_rows(win_c_ref, columns, dot_bf16(normed, query_w[...]), tap_c_ref)
    overlap = jnp.sum(keys * queries, axis=-1, keepdims=True)
    query_hi = queries.astype(jnp.bfloat16)
    query_lo = (queries - query_hi.astype(jnp.float32)).astype(jnp.bfloat16)
    row_of = lax.broadcasted_iota(jnp.int32, (ROW_TILE, width), 0)
    for b in range(blocks):
        state_copies[b].wait()
        lines = slice(b * ROW_TILE, (b + 1) * ROW_TILE)
        both = jnp.concatenate([query_hi[lines], query_lo[lines]], axis=0)
        total = jnp.zeros((ROW_TILE, width), jnp.float32)
        for i in range(ROW_TILE):
            found = dot_nt(both, state[b * ROW_TILE + i].astype(jnp.bfloat16))
            total = jnp.where(row_of == i, found[:ROW_TILE] + found[ROW_TILE:], total)
        y_ref[lines] = total
    spread = (
        lax.broadcasted_iota(jnp.int32, (HEADS, width), 0)
        == first_head + lax.broadcasted_iota(jnp.int32, (HEADS, width), 1) // HEAD_DIM
    ).astype(jnp.float32)
    copies[2].wait()
    values = conv_rows(win_x_ref, slice(None), dot_bf16(normed, value_w[...]), tap_x_ref)
    copies[3].wait()
    gate_z = dot_bf16(normed, gate_w[...])
    read_out = (
        dot_exact(decay, spread) * y_ref[...]
        + (dot_exact(step_size, spread) * overlap + dot_exact(skip_ref[...], spread)) * values
    )
    gated = read_out * silu(gate_z)
    mean_sq = dot_nt(gated * gated, spread, lax.Precision.HIGHEST) * (1.0 / HEAD_DIM)
    scale_heads = dot_exact(lax.rsqrt(mean_sq + norm_epsilon), spread)
    mixed = (gated * scale_heads * head_gain_ref[...]).astype(jnp.bfloat16)
    copies[4].wait()
    part_width = part_ref.shape[2]
    for j in range(part_ref.shape[0]):
        part_ref[j] = dot_bf16(mixed, out_w[:, j * part_width : (j + 1) * part_width]).astype(jnp.bfloat16)


def slots_of(ids_ref, experts):
    seqs = ids_ref.shape[1]
    shape = (experts * ROW_TILE, seqs)
    line = lax.broadcasted_iota(jnp.int32, shape, 0)
    expert = line // ROW_TILE
    first = ids_ref[0:1, :] == expert
    second = ids_ref[1:2, :] == expert
    hit = jnp.logical_or(first, second)
    before = (
        lax.broadcasted_iota(jnp.int32, (seqs, seqs), 0) < lax.broadcasted_iota(jnp.int32, (seqs, seqs), 1)
    ).astype(jnp.bfloat16)
    rank = dot_bf16(hit.astype(jnp.bfloat16), before)
    place = (line % ROW_TILE).astype(jnp.float32)
    return jnp.logical_and(hit, rank == place), first


def pack_body(part_ref, own_ref, ids_ref, residual_ref, outgoing_ref):
    total = own_ref[...].astype(jnp.float32)
    share = part_ref[0].astype(jnp.float32)
    for j in range(1, part_ref.shape[0]):
        share = share + part_ref[j].astype(jnp.float32)
    residual = (total + share).astype(jnp.bfloat16)
    residual_ref[...] = residual
    chosen, unused = slots_of(ids_ref, outgoing_ref.shape[0] // ROW_TILE)
    outgoing_ref[...] = dot_bf16(chosen.astype(jnp.bfloat16), residual).astype(jnp.bfloat16)


def expert_body(
    arrived_ref, gain_ref, gate_hbm, up_hbm, down_hbm, result_ref, gate_w, up_w, down_w, x_ref, sems
):
    pieces = sems.shape[1]
    copies = []
    for piece in range(pieces):
        for which, (source, target) in enumerate(((gate_hbm, gate_w), (up_hbm, up_w))):
            lines = source.shape[0] // pieces
            span = pl.ds(piece * lines, lines)
            copies.append(pltpu.make_async_copy(source.at[span], target.at[span], sems.at[which, piece]))
    lines_down = down_hbm.shape[0] // pieces
    down_copies = [
        pltpu.make_async_copy(
            down_hbm.at[pl.ds(piece * lines_down, lines_down)],
            down_w.at[pl.ds(piece * lines_down, lines_down)],
            sems.at[2, piece],
        )
        for piece in range(pieces)
    ]
    for copy in copies + down_copies:
        copy.start()
    tp_count = lax.axis_size("tp")
    ep_count = lax.axis_size("ep")
    own_width = arrived_ref.shape[1]
    for source in range(ep_count):
        for part in range(tp_count):
            x_ref[source * ROW_TILE : (source + 1) * ROW_TILE, part * own_width : (part + 1) * own_width] = (
                arrived_ref[pl.ds((source * tp_count + part) * ROW_TILE, ROW_TILE), :].astype(jnp.float32)
            )
    rows = x_ref[...]
    scale = lax.rsqrt(jnp.mean(rows * rows, axis=-1, keepdims=True) + norm_epsilon)
    ffn_in = (rows * scale * gain_ref[...]).astype(jnp.bfloat16)
    gate_part = 0.0
    up_part = 0.0
    lines = gate_hbm.shape[0] // pieces
    for piece in range(pieces):
        span = slice(piece * lines, (piece + 1) * lines)
        copies[2 * piece].wait()
        gate_part = gate_part + dot_bf16(ffn_in[:, span], gate_w[span])
        copies[2 * piece + 1].wait()
        up_part = up_part + dot_bf16(ffn_in[:, span], up_w[span])
    hidden = (silu(gate_part) * up_part).astype(jnp.bfloat16)
    result = 0.0
    for piece in range(pieces):
        span = slice(piece * lines_down, (piece + 1) * lines_down)
        down_copies[piece].wait()
        result = result + dot_bf16(hidden[:, span], down_w[span])
    for source in range(ep_count):
        for part in range(tp_count):
            result_ref[pl.ds((source * tp_count + part) * ROW_TILE, ROW_TILE), :] = result[
                source * ROW_TILE : (source + 1) * ROW_TILE, part * own_width : (part + 1) * own_width
            ].astype(jnp.bfloat16)


def combine_body(returned_ref, residual_ref, ids_ref, weight_ref, out_ref):
    chosen, first = slots_of(ids_ref, returned_ref.shape[0] // ROW_TILE)
    weights = weight_ref[...]
    share = weights / jnp.sum(weights, axis=0, keepdims=True)
    picked = jnp.where(chosen, jnp.where(first, share[0:1, :], share[1:2, :]), 0.0)
    high = picked.astype(jnp.bfloat16)
    low = (picked - high.astype(jnp.float32)).astype(jnp.bfloat16)
    returned = returned_ref[...]
    dims = (((0,), (0,)), ((), ()))
    moe_sum = lax.dot_general(high, returned, dims, preferred_element_type=jnp.float32)
    moe_sum = moe_sum + lax.dot_general(low, returned, dims, preferred_element_type=jnp.float32)
    out_ref[...] = (residual_ref[...].astype(jnp.float32) + moe_sum).astype(jnp.bfloat16)


IN_VMEM = pl.BlockSpec(memory_space=pltpu.VMEM)
IN_HBM = pl.BlockSpec(memory_space=pltpu.HBM)


def local_fast(
    tokens,
    mix_gain,
    w_gate_z,
    w_value_x,
    w_key_b,
    w_query_c,
    w_step,
    step_bias,
    decay_log,
    skip_gain,
    conv_x_weight,
    conv_b_weight,
    conv_c_weight,
    window_x,
    window_b,
    window_c,
    ssm_state,
    head_gain,
    w_out,
    ffn_gain,
    route_ids,
    route_weights,
    expert_gate,
    expert_up,
    expert_down,
):
    tp_count = lax.axis_size("tp")
    ep_count = lax.axis_size("ep")
    seqs, own_width = tokens.shape
    model_width = w_gate_z.shape[0]
    width = w_gate_z.shape[1]
    devices = ep_count * tp_count
    bf16 = jnp.bfloat16
    gathered = lax.all_gather(tokens, "tp", axis=1, tiled=True)
    parts = pl.pallas_call(
        mixer_body,
        out_shape=jax.ShapeDtypeStruct((tp_count, seqs, own_width), bf16),
        in_specs=[IN_VMEM] * 13 + [IN_HBM] * 6,
        out_specs=IN_VMEM,
        scratch_shapes=[
            pltpu.VMEM((model_width, width), bf16),
            pltpu.VMEM((model_width, width), bf16),
            pltpu.VMEM((model_width, STATE), bf16),
            pltpu.VMEM((model_width, STATE), bf16),
            pltpu.VMEM((seqs, width, STATE), jnp.float32),
            pltpu.VMEM((width, model_width), bf16),
            pltpu.VMEM((seqs, width), jnp.float32),
            pltpu.SemaphoreType.DMA((5,)),
            pltpu.SemaphoreType.DMA((seqs // ROW_TILE,)),
        ],
        name="mixer",
    )(
        gathered,
        mix_gain[None],
        w_step.T,
        step_bias[None],
        decay_log[None],
        skip_gain[None],
        conv_x_weight,
        conv_b_weight,
        conv_c_weight,
        jnp.swapaxes(window_x, 0, 1),
        jnp.swapaxes(window_b, 0, 1),
        jnp.swapaxes(window_c, 0, 1),
        head_gain[None],
        w_gate_z,
        w_value_x,
        w_key_b,
        w_query_c,
        ssm_state.reshape(seqs, width, STATE),
        w_out,
    )
    shares = lax.all_to_all(parts, "tp", split_axis=0, concat_axis=0, tiled=True)
    ids = route_ids.T
    residual, outgoing = pl.pallas_call(
        pack_body,
        out_shape=(
            jax.ShapeDtypeStruct((seqs, own_width), bf16),
            jax.ShapeDtypeStruct((devices * ROW_TILE, own_width), bf16),
        ),
        in_specs=[IN_VMEM] * 3,
        out_specs=(IN_VMEM, IN_VMEM),
        name="pack",
    )(shares, tokens, ids)

    def exchange(lines):
        split = lines.reshape(devices, ROW_TILE, own_width)
        moved = lax.all_to_all(split, ("ep", "tp"), split_axis=0, concat_axis=0, tiled=True)
        return moved.reshape(devices * ROW_TILE, own_width)

    arrived = exchange(outgoing)
    units = expert_gate.shape[2]
    result = pl.pallas_call(
        expert_body,
        out_shape=jax.ShapeDtypeStruct((devices * ROW_TILE, own_width), bf16),
        in_specs=[IN_VMEM] * 2 + [IN_HBM] * 3,
        out_specs=IN_VMEM,
        scratch_shapes=[
            pltpu.VMEM((model_width, units), bf16),
            pltpu.VMEM((model_width, units), bf16),
            pltpu.VMEM((units, model_width), bf16),
            pltpu.VMEM((ep_count * ROW_TILE, model_width), jnp.float32),
            pltpu.SemaphoreType.DMA((3, 4)),
        ],
        name="expert",
    )(arrived, ffn_gain[None], expert_gate[0], expert_up[0], expert_down[0])
    returned = exchange(result)
    return pl.pallas_call(
        combine_body,
        out_shape=jax.ShapeDtypeStruct((seqs, own_width), bf16),
        in_specs=[IN_VMEM] * 4,
        out_specs=IN_VMEM,
        name="combine",
    )(returned, residual, ids, route_weights.T)


def local(*arrays):
    tokens, w_gate_z, route_ids = arrays[0], arrays[2], arrays[20]
    seqs, own_width = tokens.shape
    width = w_gate_z.shape[1]
    tp_count = lax.axis_size("tp")
    expert_count = EXP_IN * lax.axis_size("ep")
    capacity = max(2, (3 * seqs * route_ids.shape[1] + 2 * expert_count - 1) // (2 * expert_count))
    fits = (
        tp_count == EXP_IN
        and capacity <= ROW_TILE
        and seqs % ROW_TILE == 0
        and own_width % LANES == 0
        and width % LANES == 0
    )
    return (local_fast if fits else local_generic)(*arrays)


def solution(mesh):
    in_specs = (
        P("ep", "tp"),
        P(),
        P(None, "tp"),
        P(None, "tp"),
        P(),
        P(),
        P(),
        P(),
        P(),
        P(),
        P(None, "tp"),
        P(),
        P(),
        P("ep", None, "tp"),
        P("ep", None, None),
        P("ep", None, None),
        P("ep", "tp", None, None),
        P("tp"),
        P("tp", None),
        P(),
        P("ep", None),
        P("ep", None),
        P("ep", None, "tp"),
        P("ep", None, "tp"),
        P("ep", "tp", None),
    )
    out_specs = P("ep", "tp")
    return jax.shard_map(local, mesh=mesh, in_specs=in_specs, out_specs=out_specs, check_vma=False)
```

```python
import jax
import jax.numpy as jnp
from jax import lax
from jax.experimental import pallas as pl
from jax.experimental.pallas import tpu as pltpu
from jax.sharding import PartitionSpec as P

HEADS = 32
HEAD_DIM = 64
STATE = 128
GROUPS = 2
EXP_IN = 4


norm_epsilon = 1e-06


def row_norm(arr_values, norm_gain):
    widened = arr_values.astype(jnp.float32)
    return (
        widened
        * lax.rsqrt(jnp.mean(widened * widened, axis=-1, keepdims=True) + norm_epsilon)
        * norm_gain
    )


def short_conv(window, fresh_row, weight):
    conv_taps = weight.astype(jnp.float32)
    summed = (
        jnp.sum(window.astype(jnp.float32) * conv_taps[:-1][None], axis=1)
        + fresh_row * conv_taps[-1]
    )
    return jax.nn.silu(summed)


def product(left, right):
    return jnp.dot(left, right, preferred_element_type=jnp.float32)


def local_generic(
    tokens,
    mix_gain,
    w_gate_z,
    w_value_x,
    w_key_b,
    w_query_c,
    w_step,
    step_bias,
    decay_log,
    skip_gain,
    conv_x_weight,
    conv_b_weight,
    conv_c_weight,
    window_x,
    window_b,
    window_c,
    ssm_state,
    head_gain,
    w_out,
    ffn_gain,
    route_ids,
    route_weights,
    expert_gate,
    expert_up,
    expert_down,
):
    tp_index = lax.axis_index("tp")
    tp_count = lax.axis_size("tp")
    ep_count = lax.axis_size("ep")
    seq_count = tokens.shape[0]
    gathered = lax.all_gather(tokens, "tp", axis=1, tiled=True)
    normed = row_norm(gathered, mix_gain).astype(jnp.bfloat16)
    local_width = w_gate_z.shape[1]
    head_count = local_width // HEAD_DIM
    first_head = tp_index * head_count
    group_start = first_head // (HEADS // GROUPS) * STATE
    gate_z = product(normed, w_gate_z)
    values = short_conv(window_x, product(normed, w_value_x), conv_x_weight)
    key_b = short_conv(
        lax.dynamic_slice_in_dim(window_b, group_start, STATE, 2),
        product(normed, lax.dynamic_slice_in_dim(w_key_b, group_start, STATE, 1)),
        lax.dynamic_slice_in_dim(conv_b_weight, group_start, STATE, 1),
    )
    query_c = short_conv(
        lax.dynamic_slice_in_dim(window_c, group_start, STATE, 2),
        product(normed, lax.dynamic_slice_in_dim(w_query_c, group_start, STATE, 1)),
        lax.dynamic_slice_in_dim(conv_c_weight, group_start, STATE, 1),
    )
    step_all = product(normed, w_step) + step_bias
    step_size = jax.nn.softplus(lax.dynamic_slice_in_dim(step_all, first_head, head_count, 1))
    rate_heads = jnp.exp(lax.dynamic_slice_in_dim(decay_log, first_head, head_count, 0))
    skip_heads = lax.dynamic_slice_in_dim(skip_gain, first_head, head_count, 0)
    decay_heads = jnp.exp(-step_size * rate_heads)
    value_heads = values.reshape(seq_count, head_count, HEAD_DIM)
    new_state = (
        decay_heads[:, :, None, None] * ssm_state
        + (step_size[:, :, None] * value_heads)[..., None] * key_b[:, None, None, :]
    )
    read_out = jnp.einsum("shpn,sn->shp", new_state, query_c, precision=lax.Precision.HIGHEST)
    read_out = read_out + skip_heads[None, :, None] * value_heads
    gated = read_out * jax.nn.silu(gate_z.reshape(seq_count, head_count, HEAD_DIM))
    gated = gated * lax.rsqrt(jnp.mean(gated * gated, axis=-1, keepdims=True) + norm_epsilon)
    mixed_heads = (
        (gated * head_gain.reshape(head_count, HEAD_DIM))
        .reshape(seq_count, local_width)
        .astype(jnp.bfloat16)
    )
    partial_value = product(mixed_heads, w_out)
    share_mix = lax.psum_scatter(partial_value, "tp", scatter_dimension=1, tiled=True)
    residual_own = (tokens.astype(jnp.float32) + share_mix).astype(jnp.bfloat16)
    residual_full = lax.all_gather(residual_own, "tp", axis=1, tiled=True)
    ffn_in = row_norm(residual_full, ffn_gain).astype(jnp.bfloat16)
    top_count = route_ids.shape[1]
    expert_count = EXP_IN * ep_count
    capacity = max(2, (3 * seq_count * top_count + 2 * expert_count - 1) // (2 * expert_count))
    sub_index = tp_index // (tp_count // EXP_IN)
    target_set = route_ids // EXP_IN
    hit_mask = route_ids % EXP_IN == sub_index
    set_grid = jnp.arange(ep_count, dtype=jnp.int32)
    set_onehot = (hit_mask[:, :, None] & (target_set[:, :, None] == set_grid)).astype(jnp.int32)
    set_onehot = set_onehot.reshape(seq_count * top_count, ep_count)
    earlier = jnp.cumsum(set_onehot, axis=0) - set_onehot
    slot_rank = jnp.sum(earlier * set_onehot, axis=1).reshape(seq_count, top_count)
    slot_index = jnp.where(hit_mask, target_set * capacity + slot_rank, -1)
    slot_grid = jnp.arange(ep_count * capacity, dtype=jnp.int32)
    slot_match = slot_index[:, :, None] == slot_grid
    placed = jnp.any(slot_match, axis=1).astype(jnp.bfloat16)
    outgoing = jnp.einsum("sj,sd->jd", placed, ffn_in, preferred_element_type=jnp.float32)
    outgoing = outgoing.astype(jnp.bfloat16).reshape(ep_count, capacity, ffn_in.shape[1])
    route_share = route_weights / jnp.sum(route_weights, axis=1, keepdims=True)
    combine_weight = jnp.sum(jnp.where(slot_match, route_share[:, :, None], 0.0), axis=1)
    arrived = lax.all_to_all(outgoing, "ep", split_axis=0, concat_axis=0, tiled=True)
    source_count, slot_count, row_width = arrived.shape
    flat_rows = arrived.reshape(source_count * slot_count, row_width)
    gate_part = product(flat_rows, expert_gate[0])
    up_part = product(flat_rows, expert_up[0])
    hidden = (jax.nn.silu(gate_part) * up_part).astype(jnp.bfloat16)
    expert_out = product(hidden, expert_down[0]).reshape(source_count, slot_count, row_width)
    returned = lax.all_to_all(
        expert_out.astype(jnp.bfloat16), "ep", split_axis=0, concat_axis=0, tiled=True
    ).astype(expert_out.dtype)
    moe_part = jnp.dot(
        combine_weight,
        returned.reshape(ep_count * capacity, -1),
        precision=lax.Precision.HIGHEST,
        preferred_element_type=jnp.float32,
    )
    moe_share = lax.psum_scatter(
        moe_part.astype(jnp.bfloat16), "tp", scatter_dimension=1, tiled=True
    ).astype(jnp.float32)
    return (residual_own.astype(jnp.float32) + moe_share).astype(jnp.bfloat16)


ROW_TILE = 8
LANES = 128


def dot_bf16(left, right):
    return lax.dot_general(left, right, (((1,), (0,)), ((), ())), preferred_element_type=jnp.float32)


def dot_nt(left, right, precision=None):
    return lax.dot_general(
        left, right, (((1,), (1,)), ((), ())), precision=precision, preferred_element_type=jnp.float32
    )


def dot_exact(left, right):
    return lax.dot_general(
        left,
        right,
        (((1,), (0,)), ((), ())),
        precision=lax.Precision.HIGHEST,
        preferred_element_type=jnp.float32,
    )


def silu(value):
    return value / (1.0 + jnp.exp(-value))


def conv_rows(window_ref, columns, fresh, taps_ref):
    taps = taps_ref[:, columns].astype(jnp.float32)
    count = window_ref.shape[0]
    summed = fresh * taps[count : count + 1]
    for tap in range(count):
        summed = summed + window_ref[tap, :, columns].astype(jnp.float32) * taps[tap : tap + 1]
    return silu(summed)


def mixer_body(
    row_ref,
    gain_ref,
    step_w_ref,
    bias_ref,
    rate_ref,
    skip_ref,
    tap_x_ref,
    tap_b_ref,
    tap_c_ref,
    win_x_ref,
    win_b_ref,
    win_c_ref,
    head_gain_ref,
    gate_w,
    value_w,
    key_w,
    query_w,
    state,
    out_w,
    part_ref,
    y_ref,
):
    tp_index = lax.axis_index("tp")
    seqs, width = y_ref.shape
    head_count = width // HEAD_DIM
    first_head = tp_index * head_count
    group = first_head // (HEADS // GROUPS)
    columns = pl.ds(pl.multiple_of(group * STATE, STATE), STATE)
    blocks = seqs // ROW_TILE
    rows = row_ref[...].astype(jnp.float32)
    scale = lax.rsqrt(jnp.mean(rows * rows, axis=-1, keepdims=True) + norm_epsilon)
    normed = (rows * scale * gain_ref[...]).astype(jnp.bfloat16)
    step_size = jax.nn.softplus(dot_nt(normed, step_w_ref[...]) + bias_ref[...])
    decay = jnp.exp(-step_size * jnp.exp(rate_ref[...]))
    keys = conv_rows(win_b_ref, columns, dot_bf16(normed, key_w[:, columns]), tap_b_ref)
    queries = conv_rows(win_c_ref, columns, dot_bf16(normed, query_w[:, columns]), tap_c_ref)
    overlap = jnp.sum(keys * queries, axis=-1, keepdims=True)
    query_hi = queries.astype(jnp.bfloat16)
    query_lo = (queries - query_hi.astype(jnp.float32)).astype(jnp.bfloat16)
    row_of = lax.broadcasted_iota(jnp.int32, (ROW_TILE, width), 0)
    for b in range(blocks):
        lines = slice(b * ROW_TILE, (b + 1) * ROW_TILE)
        both = jnp.concatenate([query_hi[lines], query_lo[lines]], axis=0)
        total = jnp.zeros((ROW_TILE, width), jnp.float32)
        for i in range(ROW_TILE):
            found = dot_nt(both, state[b * ROW_TILE + i].astype(jnp.bfloat16))
            total = jnp.where(row_of == i, found[:ROW_TILE] + found[ROW_TILE:], total)
        y_ref[lines] = total
    spread = (
        lax.broadcasted_iota(jnp.int32, (HEADS, width), 0)
        == first_head + lax.broadcasted_iota(jnp.int32, (HEADS, width), 1) // HEAD_DIM
    ).astype(jnp.float32)
    values = conv_rows(win_x_ref, slice(None), dot_bf16(normed, value_w[...]), tap_x_ref)
    gate_z = dot_bf16(normed, gate_w[...])
    read_out = (
        dot_exact(decay, spread) * y_ref[...]
        + (dot_exact(step_size, spread) * overlap + dot_exact(skip_ref[...], spread)) * values
    )
    gated = read_out * silu(gate_z)
    mean_sq = dot_nt(gated * gated, spread, lax.Precision.HIGHEST) * (1.0 / HEAD_DIM)
    scale_heads = dot_exact(lax.rsqrt(mean_sq + norm_epsilon), spread)
    mixed = (gated * scale_heads * head_gain_ref[...]).astype(jnp.bfloat16)
    part_width = part_ref.shape[2]
    for j in range(part_ref.shape[0]):
        part_ref[j] = dot_bf16(mixed, out_w[:, j * part_width : (j + 1) * part_width]).astype(jnp.bfloat16)


def slots_of(ids_ref, experts):
    seqs = ids_ref.shape[1]
    shape = (experts * ROW_TILE, seqs)
    line = lax.broadcasted_iota(jnp.int32, shape, 0)
    expert = line // ROW_TILE
    first = ids_ref[0:1, :] == expert
    second = ids_ref[1:2, :] == expert
    hit = jnp.logical_or(first, second)
    before = (
        lax.broadcasted_iota(jnp.int32, (seqs, seqs), 0) < lax.broadcasted_iota(jnp.int32, (seqs, seqs), 1)
    ).astype(jnp.bfloat16)
    rank = dot_bf16(hit.astype(jnp.bfloat16), before)
    place = (line % ROW_TILE).astype(jnp.float32)
    return jnp.logical_and(hit, rank == place), first


def route_body(
    own_hbm, ids_hbm, weight_hbm, own_ref, chosen_ref, high_ref, low_ref, ids_ref, weight_ref, sems
):
    copies = [
        pltpu.make_async_copy(source, target, sems.at[i])
        for i, (source, target) in enumerate(
            ((ids_hbm, ids_ref), (weight_hbm, weight_ref), (own_hbm, own_ref))
        )
    ]
    for copy in copies:
        copy.start()
    for copy in copies:
        copy.wait()
    chosen, first = slots_of(ids_ref, chosen_ref.shape[0] // ROW_TILE)
    chosen_ref[...] = chosen.astype(jnp.bfloat16)
    weights = weight_ref[...]
    share = weights / jnp.sum(weights, axis=0, keepdims=True)
    picked = jnp.where(chosen, jnp.where(first, share[0:1, :], share[1:2, :]), 0.0).T
    high = picked.astype(jnp.bfloat16)
    high_ref[...] = high
    low_ref[...] = (picked - high.astype(jnp.float32)).astype(jnp.bfloat16)


def pack_body(part_ref, own_ref, chosen_ref, residual_ref, outgoing_ref):
    share = part_ref[0].astype(jnp.float32)
    for j in range(1, part_ref.shape[0]):
        share = share + part_ref[j].astype(jnp.float32)
    residual = (own_ref[...].astype(jnp.float32) + share).astype(jnp.bfloat16)
    residual_ref[...] = residual
    outgoing_ref[...] = dot_bf16(chosen_ref[...], residual).astype(jnp.bfloat16)


def expert_body(arrived_ref, gain_ref, gate_w, up_w, down_w, result_ref, x_ref):
    tp_count = lax.axis_size("tp")
    ep_count = lax.axis_size("ep")
    own_width = arrived_ref.shape[1]
    for source in range(ep_count):
        for part in range(tp_count):
            x_ref[source * ROW_TILE : (source + 1) * ROW_TILE, part * own_width : (part + 1) * own_width] = (
                arrived_ref[pl.ds((source * tp_count + part) * ROW_TILE, ROW_TILE), :].astype(jnp.float32)
            )
    rows = x_ref[...]
    scale = lax.rsqrt(jnp.mean(rows * rows, axis=-1, keepdims=True) + norm_epsilon)
    ffn_in = (rows * scale * gain_ref[...]).astype(jnp.bfloat16)
    hidden = (silu(dot_bf16(ffn_in, gate_w[...])) * dot_bf16(ffn_in, up_w[...])).astype(jnp.bfloat16)
    result = dot_bf16(hidden, down_w[...])
    for source in range(ep_count):
        for part in range(tp_count):
            result_ref[pl.ds((source * tp_count + part) * ROW_TILE, ROW_TILE), :] = result[
                source * ROW_TILE : (source + 1) * ROW_TILE, part * own_width : (part + 1) * own_width
            ].astype(jnp.bfloat16)


def combine_body(returned_ref, residual_ref, high_ref, low_ref, out_ref):
    returned = returned_ref[...]
    moe_sum = dot_bf16(high_ref[...], returned) + dot_bf16(low_ref[...], returned)
    out_ref[...] = (residual_ref[...].astype(jnp.float32) + moe_sum).astype(jnp.bfloat16)


IN_VMEM = pl.BlockSpec(memory_space=pltpu.VMEM)
IN_HBM = pl.BlockSpec(memory_space=pltpu.HBM)


def resident(array):
    return pltpu.with_memory_space_constraint(array, pltpu.VMEM)


def grant(mebibytes):
    return pltpu.CompilerParams(vmem_limit_bytes=mebibytes * 2**20)


def local_fast(
    tokens,
    mix_gain,
    w_gate_z,
    w_value_x,
    w_key_b,
    w_query_c,
    w_step,
    step_bias,
    decay_log,
    skip_gain,
    conv_x_weight,
    conv_b_weight,
    conv_c_weight,
    window_x,
    window_b,
    window_c,
    ssm_state,
    head_gain,
    w_out,
    ffn_gain,
    route_ids,
    route_weights,
    expert_gate,
    expert_up,
    expert_down,
):
    tp_count = lax.axis_size("tp")
    ep_count = lax.axis_size("ep")
    seqs, own_width = tokens.shape
    model_width = w_gate_z.shape[0]
    width = w_gate_z.shape[1]
    devices = ep_count * tp_count
    bf16 = jnp.bfloat16
    lines = devices * ROW_TILE
    own, chosen, high, low = pl.pallas_call(
        route_body,
        out_shape=(
            pltpu.VMEM((seqs, own_width), bf16),
            pltpu.VMEM((lines, seqs), bf16),
            pltpu.VMEM((seqs, lines), bf16),
            pltpu.VMEM((seqs, lines), bf16),
        ),
        in_specs=[IN_HBM] * 3,
        out_specs=(IN_VMEM,) * 4,
        scratch_shapes=[
            pltpu.VMEM(route_ids.shape[::-1], jnp.int32),
            pltpu.VMEM(route_ids.shape[::-1], jnp.float32),
            pltpu.SemaphoreType.DMA((3,)),
        ],
        compiler_params=grant(4),
        cost_estimate=pl.CostEstimate(flops=2 * 10**10, bytes_accessed=2**25, transcendentals=0),
        name="route",
    )(
        pltpu.with_memory_space_constraint(tokens, pltpu.HBM),
        pltpu.with_memory_space_constraint(route_ids.T, pltpu.HBM),
        pltpu.with_memory_space_constraint(route_weights.T, pltpu.HBM),
    )
    gathered = lax.all_gather(own, "tp", axis=1, tiled=True)
    parts = pl.pallas_call(
        mixer_body,
        out_shape=pltpu.VMEM((tp_count, seqs, own_width), bf16),
        in_specs=[IN_VMEM] * 19,
        out_specs=IN_VMEM,
        scratch_shapes=[
            pltpu.VMEM((seqs, width), jnp.float32),
        ],
        compiler_params=grant(4),
        name="mixer",
    )(
        gathered,
        mix_gain[None],
        w_step.T,
        step_bias[None],
        decay_log[None],
        skip_gain[None],
        conv_x_weight,
        conv_b_weight,
        conv_c_weight,
        jnp.swapaxes(window_x, 0, 1),
        jnp.swapaxes(window_b, 0, 1),
        jnp.swapaxes(window_c, 0, 1),
        head_gain[None],
        resident(w_gate_z),
        resident(w_value_x),
        resident(w_key_b),
        resident(w_query_c),
        resident(ssm_state.reshape(seqs, width, STATE)),
        resident(w_out),
    )
    shares = lax.all_to_all(parts, "tp", split_axis=0, concat_axis=0, tiled=True)
    residual, outgoing = pl.pallas_call(
        pack_body,
        out_shape=(
            pltpu.VMEM((seqs, own_width), bf16),
            pltpu.VMEM((lines, own_width), bf16),
        ),
        in_specs=[IN_VMEM] * 3,
        out_specs=(IN_VMEM, IN_VMEM),
        compiler_params=grant(4),
        name="pack",
    )(shares, own, chosen)

    def exchange(sent):
        split = sent.reshape(devices, ROW_TILE, own_width)
        moved = lax.all_to_all(split, ("ep", "tp"), split_axis=0, concat_axis=0, tiled=True)
        return moved.reshape(lines, own_width)

    arrived = exchange(outgoing)
    result = pl.pallas_call(
        expert_body,
        out_shape=pltpu.VMEM((lines, own_width), bf16),
        in_specs=[IN_VMEM] * 5,
        out_specs=IN_VMEM,
        scratch_shapes=[
            pltpu.VMEM((ep_count * ROW_TILE, model_width), jnp.float32),
        ],
        compiler_params=grant(4),
        name="expert",
    )(
        arrived, ffn_gain[None], resident(expert_gate[0]), resident(expert_up[0]), resident(expert_down[0])
    )
    returned = exchange(result)
    return pl.pallas_call(
        combine_body,
        out_shape=jax.ShapeDtypeStruct((seqs, own_width), bf16),
        in_specs=[IN_VMEM] * 4,
        out_specs=IN_VMEM,
        compiler_params=grant(4),
        name="combine",
    )(returned, residual, high, low)


def local(*arrays):
    tokens, w_gate_z, route_ids = arrays[0], arrays[2], arrays[20]
    seqs, own_width = tokens.shape
    width = w_gate_z.shape[1]
    tp_count = lax.axis_size("tp")
    expert_count = EXP_IN * lax.axis_size("ep")
    capacity = max(2, (3 * seqs * route_ids.shape[1] + 2 * expert_count - 1) // (2 * expert_count))
    fits = (
        tp_count == EXP_IN
        and capacity <= ROW_TILE
        and seqs % ROW_TILE == 0
        and own_width % LANES == 0
        and width % LANES == 0
    )
    return (local_fast if fits else local_generic)(*arrays)


def solution(mesh):
    in_specs = (
        P("ep", "tp"),
        P(),
        P(None, "tp"),
        P(None, "tp"),
        P(),
        P(),
        P(),
        P(),
        P(),
        P(),
        P(None, "tp"),
        P(),
        P(),
        P("ep", None, "tp"),
        P("ep", None, None),
        P("ep", None, None),
        P("ep", "tp", None, None),
        P("tp"),
        P("tp", None),
        P(),
        P("ep", None),
        P("ep", None),
        P("ep", None, "tp"),
        P("ep", None, "tp"),
        P("ep", "tp", None),
    )
    out_specs = P("ep", "tp")
    return jax.shard_map(local, mesh=mesh, in_specs=in_specs, out_specs=out_specs, check_vma=False)
```

```python
import jax
import jax.numpy as jnp
from jax import lax
from jax.experimental import pallas as pl
from jax.experimental.pallas import tpu as pltpu
from jax.sharding import PartitionSpec as P

HEADS = 32
HEAD_DIM = 64
STATE = 128
GROUPS = 2
EXP_IN = 4


norm_epsilon = 1e-06


def row_norm(arr_values, norm_gain):
    widened = arr_values.astype(jnp.float32)
    return (
        widened
        * lax.rsqrt(jnp.mean(widened * widened, axis=-1, keepdims=True) + norm_epsilon)
        * norm_gain
    )


def short_conv(window, fresh_row, weight):
    conv_taps = weight.astype(jnp.float32)
    summed = (
        jnp.sum(window.astype(jnp.float32) * conv_taps[:-1][None], axis=1)
        + fresh_row * conv_taps[-1]
    )
    return jax.nn.silu(summed)


def product(left, right):
    return jnp.dot(left, right, preferred_element_type=jnp.float32)


def local_generic(
    tokens,
    mix_gain,
    w_gate_z,
    w_value_x,
    w_key_b,
    w_query_c,
    w_step,
    step_bias,
    decay_log,
    skip_gain,
    conv_x_weight,
    conv_b_weight,
    conv_c_weight,
    window_x,
    window_b,
    window_c,
    ssm_state,
    head_gain,
    w_out,
    ffn_gain,
    route_ids,
    route_weights,
    expert_gate,
    expert_up,
    expert_down,
):
    tp_index = lax.axis_index("tp")
    tp_count = lax.axis_size("tp")
    ep_count = lax.axis_size("ep")
    seq_count = tokens.shape[0]
    gathered = lax.all_gather(tokens, "tp", axis=1, tiled=True)
    normed = row_norm(gathered, mix_gain).astype(jnp.bfloat16)
    local_width = w_gate_z.shape[1]
    head_count = local_width // HEAD_DIM
    first_head = tp_index * head_count
    group_start = first_head // (HEADS // GROUPS) * STATE
    gate_z = product(normed, w_gate_z)
    values = short_conv(window_x, product(normed, w_value_x), conv_x_weight)
    key_b = short_conv(
        lax.dynamic_slice_in_dim(window_b, group_start, STATE, 2),
        product(normed, lax.dynamic_slice_in_dim(w_key_b, group_start, STATE, 1)),
        lax.dynamic_slice_in_dim(conv_b_weight, group_start, STATE, 1),
    )
    query_c = short_conv(
        lax.dynamic_slice_in_dim(window_c, group_start, STATE, 2),
        product(normed, lax.dynamic_slice_in_dim(w_query_c, group_start, STATE, 1)),
        lax.dynamic_slice_in_dim(conv_c_weight, group_start, STATE, 1),
    )
    step_all = product(normed, w_step) + step_bias
    step_size = jax.nn.softplus(lax.dynamic_slice_in_dim(step_all, first_head, head_count, 1))
    rate_heads = jnp.exp(lax.dynamic_slice_in_dim(decay_log, first_head, head_count, 0))
    skip_heads = lax.dynamic_slice_in_dim(skip_gain, first_head, head_count, 0)
    decay_heads = jnp.exp(-step_size * rate_heads)
    value_heads = values.reshape(seq_count, head_count, HEAD_DIM)
    new_state = (
        decay_heads[:, :, None, None] * ssm_state
        + (step_size[:, :, None] * value_heads)[..., None] * key_b[:, None, None, :]
    )
    read_out = jnp.einsum("shpn,sn->shp", new_state, query_c, precision=lax.Precision.HIGHEST)
    read_out = read_out + skip_heads[None, :, None] * value_heads
    gated = read_out * jax.nn.silu(gate_z.reshape(seq_count, head_count, HEAD_DIM))
    gated = gated * lax.rsqrt(jnp.mean(gated * gated, axis=-1, keepdims=True) + norm_epsilon)
    mixed_heads = (
        (gated * head_gain.reshape(head_count, HEAD_DIM))
        .reshape(seq_count, local_width)
        .astype(jnp.bfloat16)
    )
    partial_value = product(mixed_heads, w_out)
    share_mix = lax.psum_scatter(partial_value, "tp", scatter_dimension=1, tiled=True)
    residual_own = (tokens.astype(jnp.float32) + share_mix).astype(jnp.bfloat16)
    residual_full = lax.all_gather(residual_own, "tp", axis=1, tiled=True)
    ffn_in = row_norm(residual_full, ffn_gain).astype(jnp.bfloat16)
    top_count = route_ids.shape[1]
    expert_count = EXP_IN * ep_count
    capacity = max(2, (3 * seq_count * top_count + 2 * expert_count - 1) // (2 * expert_count))
    sub_index = tp_index // (tp_count // EXP_IN)
    target_set = route_ids // EXP_IN
    hit_mask = route_ids % EXP_IN == sub_index
    set_grid = jnp.arange(ep_count, dtype=jnp.int32)
    set_onehot = (hit_mask[:, :, None] & (target_set[:, :, None] == set_grid)).astype(jnp.int32)
    set_onehot = set_onehot.reshape(seq_count * top_count, ep_count)
    earlier = jnp.cumsum(set_onehot, axis=0) - set_onehot
    slot_rank = jnp.sum(earlier * set_onehot, axis=1).reshape(seq_count, top_count)
    slot_index = jnp.where(hit_mask, target_set * capacity + slot_rank, -1)
    slot_grid = jnp.arange(ep_count * capacity, dtype=jnp.int32)
    slot_match = slot_index[:, :, None] == slot_grid
    placed = jnp.any(slot_match, axis=1).astype(jnp.bfloat16)
    outgoing = jnp.einsum("sj,sd->jd", placed, ffn_in, preferred_element_type=jnp.float32)
    outgoing = outgoing.astype(jnp.bfloat16).reshape(ep_count, capacity, ffn_in.shape[1])
    route_share = route_weights / jnp.sum(route_weights, axis=1, keepdims=True)
    combine_weight = jnp.sum(jnp.where(slot_match, route_share[:, :, None], 0.0), axis=1)
    arrived = lax.all_to_all(outgoing, "ep", split_axis=0, concat_axis=0, tiled=True)
    source_count, slot_count, row_width = arrived.shape
    flat_rows = arrived.reshape(source_count * slot_count, row_width)
    gate_part = product(flat_rows, expert_gate[0])
    up_part = product(flat_rows, expert_up[0])
    hidden = (jax.nn.silu(gate_part) * up_part).astype(jnp.bfloat16)
    expert_out = product(hidden, expert_down[0]).reshape(source_count, slot_count, row_width)
    returned = lax.all_to_all(
        expert_out.astype(jnp.bfloat16), "ep", split_axis=0, concat_axis=0, tiled=True
    ).astype(expert_out.dtype)
    moe_part = jnp.dot(
        combine_weight,
        returned.reshape(ep_count * capacity, -1),
        precision=lax.Precision.HIGHEST,
        preferred_element_type=jnp.float32,
    )
    moe_share = lax.psum_scatter(
        moe_part.astype(jnp.bfloat16), "tp", scatter_dimension=1, tiled=True
    ).astype(jnp.float32)
    return (residual_own.astype(jnp.float32) + moe_share).astype(jnp.bfloat16)


ROW_TILE = 8
LANES = 128


def dot_bf16(left, right):
    return lax.dot_general(left, right, (((1,), (0,)), ((), ())), preferred_element_type=jnp.float32)


def dot_nt(left, right, precision=None):
    return lax.dot_general(
        left, right, (((1,), (1,)), ((), ())), precision=precision, preferred_element_type=jnp.float32
    )


def dot_exact(left, right):
    return lax.dot_general(
        left,
        right,
        (((1,), (0,)), ((), ())),
        precision=lax.Precision.HIGHEST,
        preferred_element_type=jnp.float32,
    )


def silu(value):
    return value / (1.0 + jnp.exp(-value))


def conv_rows(window_ref, columns, fresh, taps_ref):
    taps = taps_ref[:, columns].astype(jnp.float32)
    count = window_ref.shape[0]
    summed = fresh * taps[count : count + 1]
    for tap in range(count):
        summed = summed + window_ref[tap, :, columns].astype(jnp.float32) * taps[tap : tap + 1]
    return silu(summed)


def mixer_body(
    own_ref,
    piece_refs,
    gain_ref,
    step_w_ref,
    bias_ref,
    rate_ref,
    skip_ref,
    tap_x_ref,
    tap_b_ref,
    tap_c_ref,
    win_x_ref,
    win_b_ref,
    win_c_ref,
    head_gain_ref,
    gate_w,
    value_w,
    key_w,
    query_w,
    state,
    out_w,
    part_refs,
    y_ref,
    row_ref,
):
    tp_index = lax.axis_index("tp")
    seqs, width = y_ref.shape
    head_count = width // HEAD_DIM
    first_head = tp_index * head_count
    group = first_head // (HEADS // GROUPS)
    columns = pl.ds(pl.multiple_of(group * STATE, STATE), STATE)
    blocks = seqs // ROW_TILE
    own_width = own_ref.shape[1]
    for k, piece_ref in enumerate((own_ref, *piece_refs)):
        row_ref[:, pl.ds(pl.multiple_of((tp_index ^ k) * own_width, own_width), own_width)] = piece_ref[...]
    rows = row_ref[...].astype(jnp.float32)
    scale = lax.rsqrt(jnp.mean(rows * rows, axis=-1, keepdims=True) + norm_epsilon)
    normed = (rows * scale * gain_ref[...]).astype(jnp.bfloat16)
    step_size = jax.nn.softplus(dot_nt(normed, step_w_ref[...]) + bias_ref[...])
    decay = jnp.exp(-step_size * jnp.exp(rate_ref[...]))
    keys = conv_rows(win_b_ref, columns, dot_bf16(normed, key_w[:, columns]), tap_b_ref)
    queries = conv_rows(win_c_ref, columns, dot_bf16(normed, query_w[:, columns]), tap_c_ref)
    overlap = jnp.sum(keys * queries, axis=-1, keepdims=True)
    query_hi = queries.astype(jnp.bfloat16)
    query_lo = (queries - query_hi.astype(jnp.float32)).astype(jnp.bfloat16)
    row_of = lax.broadcasted_iota(jnp.int32, (ROW_TILE, width), 0)
    for b in range(blocks):
        lines = slice(b * ROW_TILE, (b + 1) * ROW_TILE)
        both = jnp.concatenate([query_hi[lines], query_lo[lines]], axis=0)
        total = jnp.zeros((ROW_TILE, width), jnp.float32)
        for i in range(ROW_TILE):
            found = dot_nt(both, state[b * ROW_TILE + i].astype(jnp.bfloat16))
            total = jnp.where(row_of == i, found[:ROW_TILE] + found[ROW_TILE:], total)
        y_ref[lines] = total
    spread = (
        lax.broadcasted_iota(jnp.int32, (HEADS, width), 0)
        == first_head + lax.broadcasted_iota(jnp.int32, (HEADS, width), 1) // HEAD_DIM
    ).astype(jnp.float32)
    values = conv_rows(win_x_ref, slice(None), dot_bf16(normed, value_w[...]), tap_x_ref)
    gate_z = dot_bf16(normed, gate_w[...])
    read_out = (
        dot_exact(decay, spread) * y_ref[...]
        + (dot_exact(step_size, spread) * overlap + dot_exact(skip_ref[...], spread)) * values
    )
    gated = read_out * silu(gate_z)
    mean_sq = dot_nt(gated * gated, spread, lax.Precision.HIGHEST) * (1.0 / HEAD_DIM)
    scale_heads = dot_exact(lax.rsqrt(mean_sq + norm_epsilon), spread)
    mixed = (gated * scale_heads * head_gain_ref[...]).astype(jnp.bfloat16)
    for k, part_ref in enumerate(part_refs):
        span = pl.ds(pl.multiple_of((tp_index ^ k) * own_width, own_width), own_width)
        part_ref[...] = dot_bf16(mixed, out_w[:, span]).astype(part_ref.dtype)


def slots_of(ids_ref, experts, lines):
    seqs = ids_ref.shape[1]
    line = lax.broadcasted_iota(jnp.int32, (lines, seqs), 0)
    expert = line % experts
    first = ids_ref[0:1, :] == expert
    second = ids_ref[1:2, :] == expert
    hit = jnp.logical_or(first, second)
    before = (
        lax.broadcasted_iota(jnp.int32, (seqs, seqs), 0) < lax.broadcasted_iota(jnp.int32, (seqs, seqs), 1)
    ).astype(jnp.bfloat16)
    rank = dot_bf16(hit.astype(jnp.bfloat16), before)
    place = (line // experts).astype(jnp.float32)
    return jnp.logical_and(hit, rank == place), first


def entry_body(own_hbm, own_ref, sem):
    copy = pltpu.make_async_copy(own_hbm, own_ref, sem)
    copy.start()
    copy.wait()


def route_body(ids_ref, weight_ref, chosen_ref, high_ref, low_ref):
    experts = EXP_IN * lax.axis_size("ep")
    chosen, first = slots_of(ids_ref, experts, chosen_ref.shape[0])
    chosen_ref[...] = chosen.astype(jnp.bfloat16)
    weights = weight_ref[...]
    share = weights / jnp.sum(weights, axis=0, keepdims=True)
    picked = jnp.where(chosen, jnp.where(first, share[0:1, :], share[1:2, :]), 0.0).T
    high = picked.astype(jnp.bfloat16)
    high_ref[...] = high
    low_ref[...] = (picked - high.astype(jnp.float32)).astype(jnp.bfloat16)


def write_blocks(line_ref, moved_ref):
    devices, blocks, width = moved_ref.shape
    for d in range(devices):
        for k in range(width // LANES):
            moved_ref[d, :, k * LANES : (k + 1) * LANES] = line_ref[
                k, d * blocks : (d + 1) * blocks
            ].astype(moved_ref.dtype)


def read_blocks(moved_ref, line_ref):
    devices, blocks, width = moved_ref.shape
    for d in range(devices):
        for k in range(width // LANES):
            line_ref[k, d * blocks : (d + 1) * blocks] = moved_ref[
                d, :, k * LANES : (k + 1) * LANES
            ].astype(line_ref.dtype)


def pack_body(own_ref, part_refs, chosen_ref, residual_ref, outgoing_ref, line_ref):
    share = own_ref[...].astype(jnp.float32)
    for part_ref in part_refs:
        share = share + part_ref[...].astype(jnp.float32)
    residual = share.astype(jnp.bfloat16)
    residual_ref[...] = residual
    rows = dot_bf16(chosen_ref[...], residual)
    devices, blocks, width = outgoing_ref.shape
    for k in range(width // LANES):
        for j in range(blocks):
            line_ref[k, pl.ds(j, devices, stride=blocks)] = rows[
                k * devices : (k + 1) * devices, j * LANES : (j + 1) * LANES
            ]
    write_blocks(line_ref, outgoing_ref)


def expert_body(arrived_ref, gain_ref, gate_w, up_w, down_w, result_ref, x_ref, line_ref):
    tp_count = lax.axis_size("tp")
    ep_count = lax.axis_size("ep")
    devices, blocks, width = arrived_ref.shape
    own_width = blocks * LANES
    read_blocks(arrived_ref, line_ref)
    places = [
        (
            slice(k * ep_count, (k + 1) * ep_count),
            slice(part * own_width + j * LANES, part * own_width + (j + 1) * LANES),
            pl.ds(part * blocks + j, ep_count, stride=tp_count * blocks),
            k,
        )
        for k in range(width // LANES)
        for part in range(tp_count)
        for j in range(blocks)
    ]
    for row, column, line, k in places:
        x_ref[row, column] = line_ref[k, line]
    rows = x_ref[...]
    scale = lax.rsqrt(jnp.mean(rows * rows, axis=-1, keepdims=True) + norm_epsilon)
    ffn_in = (rows * scale * gain_ref[...]).astype(jnp.bfloat16)
    hidden = (silu(dot_bf16(ffn_in, gate_w[...])) * dot_bf16(ffn_in, up_w[...])).astype(jnp.bfloat16)
    result = dot_bf16(hidden, down_w[...])
    for row, column, line, k in places:
        line_ref[k, line] = result[row, column]
    write_blocks(line_ref, result_ref)


def combine_body(returned_ref, residual_ref, high_ref, low_ref, out_ref, line_ref):
    devices, blocks, width = returned_ref.shape
    read_blocks(returned_ref, line_ref)
    for j in range(blocks):
        rows = jnp.concatenate(
            [
                line_ref[k, pl.ds(j, devices, stride=blocks)]
                for k in range(width // LANES)
            ],
            axis=0,
        ).astype(jnp.bfloat16)
        moe_sum = dot_bf16(high_ref[...], rows) + dot_bf16(low_ref[...], rows)
        span = slice(j * LANES, (j + 1) * LANES)
        out_ref[:, span] = (residual_ref[:, span].astype(jnp.float32) + moe_sum).astype(jnp.bfloat16)


IN_VMEM = pl.BlockSpec(memory_space=pltpu.VMEM)
IN_HBM = pl.BlockSpec(memory_space=pltpu.HBM)


def resident(array):
    return pltpu.with_memory_space_constraint(array, pltpu.VMEM)


def grant(mebibytes):
    return pltpu.CompilerParams(vmem_limit_bytes=mebibytes * 2**20)


def local_fast(
    tokens,
    mix_gain,
    w_gate_z,
    w_value_x,
    w_key_b,
    w_query_c,
    w_step,
    step_bias,
    decay_log,
    skip_gain,
    conv_x_weight,
    conv_b_weight,
    conv_c_weight,
    window_x,
    window_b,
    window_c,
    ssm_state,
    head_gain,
    w_out,
    ffn_gain,
    route_ids,
    route_weights,
    expert_gate,
    expert_up,
    expert_down,
):
    tp_count = lax.axis_size("tp")
    ep_count = lax.axis_size("ep")
    seqs, own_width = tokens.shape
    model_width = w_gate_z.shape[0]
    width = w_gate_z.shape[1]
    devices = ep_count * tp_count
    bf16 = jnp.bfloat16
    f32 = jnp.float32
    capacity = capacity_of(seqs, route_ids.shape[1], devices)
    blocks = own_width // LANES
    lines = devices * capacity
    moved_shape = (devices, blocks, capacity * LANES)
    line_scratch = pltpu.VMEM((capacity, devices * blocks, LANES), f32)

    def shift(array, k):
        return lax.ppermute(array, "tp", [(i, i ^ k) for i in range(tp_count)])

    own = pl.pallas_call(
        entry_body,
        out_shape=pltpu.VMEM((seqs, own_width), bf16),
        in_specs=[IN_HBM],
        out_specs=IN_VMEM,
        scratch_shapes=[pltpu.SemaphoreType.DMA],
        compiler_params=grant(4),
        cost_estimate=pl.CostEstimate(flops=2 * 10**10, bytes_accessed=2**25, transcendentals=0),
        name="entry",
    )(pltpu.with_memory_space_constraint(tokens, pltpu.HBM))
    pieces = tuple(shift(own, k) for k in range(1, tp_count))
    chosen, high, low = pl.pallas_call(
        route_body,
        out_shape=(
            pltpu.VMEM((lines, seqs), bf16),
            pltpu.VMEM((seqs, lines), bf16),
            pltpu.VMEM((seqs, lines), bf16),
        ),
        in_specs=[IN_VMEM] * 2,
        out_specs=(IN_VMEM,) * 3,
        compiler_params=grant(4),
        cost_estimate=pl.CostEstimate(flops=10**10, bytes_accessed=2**24, transcendentals=0),
        name="route",
    )(route_ids.T, route_weights.T)
    (parts,) = pl.pallas_call(
        mixer_body,
        out_shape=(
            (pltpu.VMEM((seqs, own_width), f32),) + (pltpu.VMEM((seqs, own_width), bf16),) * (tp_count - 1),
        ),
        in_specs=[IN_VMEM, (IN_VMEM,) * (tp_count - 1)] + [IN_VMEM] * 18,
        out_specs=((IN_VMEM,) * tp_count,),
        scratch_shapes=[
            pltpu.VMEM((seqs, width), f32),
            pltpu.VMEM((seqs, model_width), bf16),
        ],
        compiler_params=grant(4),
        name="mixer",
    )(
        own,
        pieces,
        mix_gain[None],
        w_step.T,
        step_bias[None],
        decay_log[None],
        skip_gain[None],
        conv_x_weight,
        conv_b_weight,
        conv_c_weight,
        jnp.swapaxes(window_x, 0, 1),
        jnp.swapaxes(window_b, 0, 1),
        jnp.swapaxes(window_c, 0, 1),
        head_gain[None],
        resident(w_gate_z),
        resident(w_value_x),
        resident(w_key_b),
        resident(w_query_c),
        resident(ssm_state.reshape(seqs, width, STATE)),
        resident(w_out),
    )
    shares = (parts[0],) + tuple(shift(parts[k], k) for k in range(1, tp_count))
    residual, outgoing = pl.pallas_call(
        pack_body,
        out_shape=(pltpu.VMEM((seqs, own_width), bf16), pltpu.VMEM(moved_shape, bf16)),
        in_specs=[IN_VMEM, (IN_VMEM,) * tp_count, IN_VMEM],
        out_specs=(IN_VMEM, IN_VMEM),
        scratch_shapes=[line_scratch],
        compiler_params=grant(4),
        name="pack",
    )(own, shares, chosen)

    def exchange(sent):
        return lax.all_to_all(sent, ("ep", "tp"), split_axis=0, concat_axis=0, tiled=True)

    result = pl.pallas_call(
        expert_body,
        out_shape=pltpu.VMEM(moved_shape, bf16),
        in_specs=[IN_VMEM] * 5,
        out_specs=IN_VMEM,
        scratch_shapes=[pltpu.VMEM((ep_count * capacity, model_width), f32), line_scratch],
        compiler_params=grant(4),
        name="expert",
    )(
        exchange(outgoing),
        ffn_gain[None],
        resident(expert_gate[0]),
        resident(expert_up[0]),
        resident(expert_down[0]),
    )
    return pl.pallas_call(
        combine_body,
        out_shape=jax.ShapeDtypeStruct((seqs, own_width), bf16),
        in_specs=[IN_VMEM] * 4,
        out_specs=IN_VMEM,
        scratch_shapes=[line_scratch],
        compiler_params=grant(4),
        name="combine",
    )(exchange(result), residual, high, low)


def capacity_of(seqs, top_count, experts):
    return max(2, (3 * seqs * top_count + 2 * experts - 1) // (2 * experts))


def local(*arrays):
    tokens, w_gate_z = arrays[0], arrays[2]
    seqs, own_width = tokens.shape
    width = w_gate_z.shape[1]
    tp_count = lax.axis_size("tp")
    fits = (
        tp_count == EXP_IN
        and lax.axis_size("ep") % ROW_TILE == 0
        and seqs % ROW_TILE == 0
        and own_width % LANES == 0
        and width % LANES == 0
    )
    return (local_fast if fits else local_generic)(*arrays)


def solution(mesh):
    in_specs = (
        P("ep", "tp"),
        P(),
        P(None, "tp"),
        P(None, "tp"),
        P(),
        P(),
        P(),
        P(),
        P(),
        P(),
        P(None, "tp"),
        P(),
        P(),
        P("ep", None, "tp"),
        P("ep", None, None),
        P("ep", None, None),
        P("ep", "tp", None, None),
        P("tp"),
        P("tp", None),
        P(),
        P("ep", None),
        P("ep", None),
        P("ep", None, "tp"),
        P("ep", None, "tp"),
        P("ep", "tp", None),
    )
    out_specs = P("ep", "tp")
    return jax.shard_map(local, mesh=mesh, in_specs=in_specs, out_specs=out_specs, check_vma=False)
```

```python
import jax
import jax.numpy as jnp
from jax import lax
from jax.experimental import pallas as pl
from jax.experimental.pallas import tpu as pltpu
from jax.sharding import PartitionSpec as P

HEADS = 32
HEAD_DIM = 64
STATE = 128
GROUPS = 2
EXP_IN = 4


norm_epsilon = 1e-06


def row_norm(arr_values, norm_gain):
    widened = arr_values.astype(jnp.float32)
    return (
        widened
        * lax.rsqrt(jnp.mean(widened * widened, axis=-1, keepdims=True) + norm_epsilon)
        * norm_gain
    )


def short_conv(window, fresh_row, weight):
    conv_taps = weight.astype(jnp.float32)
    summed = (
        jnp.sum(window.astype(jnp.float32) * conv_taps[:-1][None], axis=1)
        + fresh_row * conv_taps[-1]
    )
    return jax.nn.silu(summed)


def product(left, right):
    return jnp.dot(left, right, preferred_element_type=jnp.float32)


def local_generic(
    tokens,
    mix_gain,
    w_gate_z,
    w_value_x,
    w_key_b,
    w_query_c,
    w_step,
    step_bias,
    decay_log,
    skip_gain,
    conv_x_weight,
    conv_b_weight,
    conv_c_weight,
    window_x,
    window_b,
    window_c,
    ssm_state,
    head_gain,
    w_out,
    ffn_gain,
    route_ids,
    route_weights,
    expert_gate,
    expert_up,
    expert_down,
):
    tp_index = lax.axis_index("tp")
    tp_count = lax.axis_size("tp")
    ep_count = lax.axis_size("ep")
    seq_count = tokens.shape[0]
    gathered = lax.all_gather(tokens, "tp", axis=1, tiled=True)
    normed = row_norm(gathered, mix_gain).astype(jnp.bfloat16)
    local_width = w_gate_z.shape[1]
    head_count = local_width // HEAD_DIM
    first_head = tp_index * head_count
    group_start = first_head // (HEADS // GROUPS) * STATE
    gate_z = product(normed, w_gate_z)
    values = short_conv(window_x, product(normed, w_value_x), conv_x_weight)
    key_b = short_conv(
        lax.dynamic_slice_in_dim(window_b, group_start, STATE, 2),
        product(normed, lax.dynamic_slice_in_dim(w_key_b, group_start, STATE, 1)),
        lax.dynamic_slice_in_dim(conv_b_weight, group_start, STATE, 1),
    )
    query_c = short_conv(
        lax.dynamic_slice_in_dim(window_c, group_start, STATE, 2),
        product(normed, lax.dynamic_slice_in_dim(w_query_c, group_start, STATE, 1)),
        lax.dynamic_slice_in_dim(conv_c_weight, group_start, STATE, 1),
    )
    step_all = product(normed, w_step) + step_bias
    step_size = jax.nn.softplus(lax.dynamic_slice_in_dim(step_all, first_head, head_count, 1))
    rate_heads = jnp.exp(lax.dynamic_slice_in_dim(decay_log, first_head, head_count, 0))
    skip_heads = lax.dynamic_slice_in_dim(skip_gain, first_head, head_count, 0)
    decay_heads = jnp.exp(-step_size * rate_heads)
    value_heads = values.reshape(seq_count, head_count, HEAD_DIM)
    new_state = (
        decay_heads[:, :, None, None] * ssm_state
        + (step_size[:, :, None] * value_heads)[..., None] * key_b[:, None, None, :]
    )
    read_out = jnp.einsum("shpn,sn->shp", new_state, query_c, precision=lax.Precision.HIGHEST)
    read_out = read_out + skip_heads[None, :, None] * value_heads
    gated = read_out * jax.nn.silu(gate_z.reshape(seq_count, head_count, HEAD_DIM))
    gated = gated * lax.rsqrt(jnp.mean(gated * gated, axis=-1, keepdims=True) + norm_epsilon)
    mixed_heads = (
        (gated * head_gain.reshape(head_count, HEAD_DIM))
        .reshape(seq_count, local_width)
        .astype(jnp.bfloat16)
    )
    partial_value = product(mixed_heads, w_out)
    share_mix = lax.psum_scatter(partial_value, "tp", scatter_dimension=1, tiled=True)
    residual_own = (tokens.astype(jnp.float32) + share_mix).astype(jnp.bfloat16)
    residual_full = lax.all_gather(residual_own, "tp", axis=1, tiled=True)
    ffn_in = row_norm(residual_full, ffn_gain).astype(jnp.bfloat16)
    top_count = route_ids.shape[1]
    expert_count = EXP_IN * ep_count
    capacity = max(2, (3 * seq_count * top_count + 2 * expert_count - 1) // (2 * expert_count))
    sub_index = tp_index // (tp_count // EXP_IN)
    target_set = route_ids // EXP_IN
    hit_mask = route_ids % EXP_IN == sub_index
    set_grid = jnp.arange(ep_count, dtype=jnp.int32)
    set_onehot = (hit_mask[:, :, None] & (target_set[:, :, None] == set_grid)).astype(jnp.int32)
    set_onehot = set_onehot.reshape(seq_count * top_count, ep_count)
    earlier = jnp.cumsum(set_onehot, axis=0) - set_onehot
    slot_rank = jnp.sum(earlier * set_onehot, axis=1).reshape(seq_count, top_count)
    slot_index = jnp.where(hit_mask, target_set * capacity + slot_rank, -1)
    slot_grid = jnp.arange(ep_count * capacity, dtype=jnp.int32)
    slot_match = slot_index[:, :, None] == slot_grid
    placed = jnp.any(slot_match, axis=1).astype(jnp.bfloat16)
    outgoing = jnp.einsum("sj,sd->jd", placed, ffn_in, preferred_element_type=jnp.float32)
    outgoing = outgoing.astype(jnp.bfloat16).reshape(ep_count, capacity, ffn_in.shape[1])
    route_share = route_weights / jnp.sum(route_weights, axis=1, keepdims=True)
    combine_weight = jnp.sum(jnp.where(slot_match, route_share[:, :, None], 0.0), axis=1)
    arrived = lax.all_to_all(outgoing, "ep", split_axis=0, concat_axis=0, tiled=True)
    source_count, slot_count, row_width = arrived.shape
    flat_rows = arrived.reshape(source_count * slot_count, row_width)
    gate_part = product(flat_rows, expert_gate[0])
    up_part = product(flat_rows, expert_up[0])
    hidden = (jax.nn.silu(gate_part) * up_part).astype(jnp.bfloat16)
    expert_out = product(hidden, expert_down[0]).reshape(source_count, slot_count, row_width)
    returned = lax.all_to_all(
        expert_out.astype(jnp.bfloat16), "ep", split_axis=0, concat_axis=0, tiled=True
    ).astype(expert_out.dtype)
    moe_part = jnp.dot(
        combine_weight,
        returned.reshape(ep_count * capacity, -1),
        precision=lax.Precision.HIGHEST,
        preferred_element_type=jnp.float32,
    )
    moe_share = lax.psum_scatter(
        moe_part.astype(jnp.bfloat16), "tp", scatter_dimension=1, tiled=True
    ).astype(jnp.float32)
    return (residual_own.astype(jnp.float32) + moe_share).astype(jnp.bfloat16)


ROW_TILE = 8
LANES = 128
VECTOR_SEQS = 16


def dot_bf16(left, right):
    return lax.dot_general(left, right, (((1,), (0,)), ((), ())), preferred_element_type=jnp.float32)


def dot_nt(left, right):
    return lax.dot_general(left, right, (((1,), (1,)), ((), ())), preferred_element_type=jnp.float32)


def halves(array):
    high = array.astype(jnp.bfloat16)
    return high, (array - high.astype(jnp.float32)).astype(jnp.bfloat16)


def silu(value):
    return value / (1.0 + jnp.exp(-value))


def conv_rows(window_ref, columns, fresh, taps_ref):
    taps = taps_ref[:, columns].astype(jnp.float32)
    count = window_ref.shape[0]
    summed = fresh * taps[count : count + 1]
    for tap in range(count):
        summed = summed + window_ref[tap, :, columns].astype(jnp.float32) * taps[tap : tap + 1]
    return silu(summed)


def mixer_body(
    own_ref,
    piece_refs,
    gain_ref,
    step_w_ref,
    bias_ref,
    rate_ref,
    skip_ref,
    tap_x_ref,
    tap_b_ref,
    tap_c_ref,
    win_x_ref,
    win_b_ref,
    win_c_ref,
    head_gain_ref,
    gate_w,
    value_w,
    key_w,
    query_w,
    state,
    out_w,
    part_refs,
    y_ref,
    row_ref,
    query_ref,
):
    tp_index = lax.axis_index("tp")
    seqs, width = y_ref.shape
    head_count = width // HEAD_DIM
    first_head = tp_index * head_count
    group = first_head // (HEADS // GROUPS)
    columns = pl.ds(pl.multiple_of(group * STATE, STATE), STATE)
    blocks = seqs // ROW_TILE
    own_width = own_ref.shape[1]
    for k, piece_ref in enumerate((own_ref, *piece_refs)):
        row_ref[:, pl.ds(pl.multiple_of((tp_index ^ k) * own_width, own_width), own_width)] = piece_ref[...]
    rows = row_ref[...].astype(jnp.float32)
    scale = lax.rsqrt(jnp.mean(rows * rows, axis=-1, keepdims=True) + norm_epsilon)
    normed = (rows * scale * gain_ref[...]).astype(jnp.bfloat16)
    step_size = jax.nn.softplus(dot_nt(normed, step_w_ref[...]) + bias_ref[...])
    decay = jnp.exp(-step_size * jnp.exp(rate_ref[...]))
    key_row = dot_bf16(normed, key_w[:, columns])
    query_row = dot_bf16(normed, query_w[:, columns])
    value_row = dot_bf16(normed, value_w[...])
    gate_z = dot_bf16(normed, gate_w[...])
    keys = conv_rows(win_b_ref, columns, key_row, tap_b_ref)
    queries = conv_rows(win_c_ref, columns, query_row, tap_c_ref)
    overlap = jnp.sum(keys * queries, axis=-1, keepdims=True)
    query_hi, query_lo = halves(queries)
    row_of = lax.broadcasted_iota(jnp.int32, (ROW_TILE, width), 0)
    lane = lax.broadcasted_iota(jnp.int32, (LANES, LANES), 1)
    query_ref[...] = queries
    first_block = VECTOR_SEQS // ROW_TILE
    for b in range(max(blocks - first_block, width // LANES)):
        if b < width // LANES:
            span = slice(b * LANES, (b + 1) * LANES)
            turned = jnp.zeros((LANES, LANES), jnp.float32)
            for i in range(VECTOR_SEQS):
                summed = jnp.sum(state[i, span] * query_ref[i : i + 1], axis=-1, keepdims=True)
                turned = jnp.where(lane == i, summed, turned)
            y_ref[:VECTOR_SEQS, span] = turned.T[:VECTOR_SEQS]
        if first_block + b < blocks:
            start = (first_block + b) * ROW_TILE
            lines = slice(start, start + ROW_TILE)
            both = jnp.concatenate([query_hi[lines], query_lo[lines]], axis=0)
            total = jnp.zeros((ROW_TILE, width), jnp.float32)
            for i in range(ROW_TILE):
                found = dot_nt(both, state[start + i].astype(jnp.bfloat16))
                total = jnp.where(row_of == i, found[:ROW_TILE] + found[ROW_TILE:], total)
            y_ref[lines] = total
    spread = (
        lax.broadcasted_iota(jnp.int32, (2 * HEADS, width), 0) % HEADS
        == first_head + lax.broadcasted_iota(jnp.int32, (2 * HEADS, width), 1) // HEAD_DIM
    ).astype(jnp.bfloat16)
    per_head = jnp.concatenate(
        [decay, step_size, jnp.broadcast_to(skip_ref[...], (ROW_TILE, HEADS))], axis=0
    )
    wide = dot_bf16(jnp.concatenate(halves(per_head), axis=1), spread)
    values = conv_rows(win_x_ref, slice(None), value_row, tap_x_ref)
    read_out = wide[:seqs] * y_ref[...] + (wide[seqs : 2 * seqs] * overlap + wide[2 * seqs : 2 * seqs + 1]) * values
    gated = read_out * silu(gate_z)
    same_head = (
        lax.broadcasted_iota(jnp.int32, (LANES, LANES), 0) // HEAD_DIM
        == lax.broadcasted_iota(jnp.int32, (LANES, LANES), 1) // HEAD_DIM
    ).astype(jnp.bfloat16)
    scaled = []
    for j in range(0, width, LANES):
        block = gated[:, j : j + LANES]
        sums = dot_bf16(jnp.concatenate(halves(block * block), axis=0), same_head)
        mean_sq = (sums[:seqs] + sums[seqs:]) * (1.0 / HEAD_DIM)
        scaled.append(block * lax.rsqrt(mean_sq + norm_epsilon) * head_gain_ref[:, j : j + LANES])
    mixed = jnp.concatenate(scaled, axis=1).astype(jnp.bfloat16)
    for k, part_ref in enumerate(part_refs):
        span = pl.ds(pl.multiple_of((tp_index ^ k) * own_width, own_width), own_width)
        part_ref[...] = dot_bf16(mixed, out_w[:, span]).astype(part_ref.dtype)


def slots_of(ids_ref, experts, lines):
    seqs = ids_ref.shape[1]
    line = lax.broadcasted_iota(jnp.int32, (lines, seqs), 0)
    sets = lax.axis_size("ep")
    expert = line % sets * EXP_IN + line % experts // sets
    first = ids_ref[0:1, :] == expert
    second = ids_ref[1:2, :] == expert
    hit = jnp.logical_or(first, second)
    before = (
        lax.broadcasted_iota(jnp.int32, (seqs, seqs), 0) < lax.broadcasted_iota(jnp.int32, (seqs, seqs), 1)
    ).astype(jnp.bfloat16)
    rank = dot_bf16(hit.astype(jnp.bfloat16), before)
    place = (line // experts).astype(jnp.float32)
    return jnp.logical_and(hit, rank == place), first


def entry_body(own_hbm, own_ref, sems):
    copies = []
    for i in range(sems.shape[0]):
        span = pl.ds(i * ROW_TILE, ROW_TILE)
        copies.append(pltpu.make_async_copy(own_hbm.at[span], own_ref.at[span], sems.at[i]))
    for copy in copies:
        copy.start()
    for copy in copies:
        copy.wait()


def route_body(ids_ref, weight_ref, chosen_ref, high_ref, low_ref):
    experts = EXP_IN * lax.axis_size("ep")
    chosen, first = slots_of(ids_ref, experts, chosen_ref.shape[0])
    chosen_ref[...] = chosen.astype(jnp.bfloat16)
    weights = weight_ref[...]
    share = weights / jnp.sum(weights, axis=0, keepdims=True)
    picked = jnp.where(chosen, jnp.where(first, share[0:1, :], share[1:2, :]), 0.0).T
    high_ref[...], low_ref[...] = halves(picked)


def write_blocks(line_ref, moved_ref):
    devices, blocks, width = moved_ref.shape
    for d in range(devices):
        for k in range(width // LANES):
            moved_ref[d, :, k * LANES : (k + 1) * LANES] = line_ref[
                k, d * blocks : (d + 1) * blocks
            ].astype(moved_ref.dtype)


def read_blocks(moved_ref, line_ref):
    devices, blocks, width = moved_ref.shape
    for d in range(devices):
        for k in range(width // LANES):
            line_ref[k, d * blocks : (d + 1) * blocks] = moved_ref[
                d, :, k * LANES : (k + 1) * LANES
            ].astype(line_ref.dtype)


def pack_body(own_ref, part_refs, chosen_ref, residual_ref, outgoing_ref, line_ref):
    share = own_ref[...].astype(jnp.float32)
    for part_ref in part_refs:
        share = share + part_ref[...].astype(jnp.float32)
    residual = share.astype(jnp.bfloat16)
    residual_ref[...] = residual
    rows = dot_bf16(chosen_ref[...], residual)
    devices, blocks, width = outgoing_ref.shape
    for k in range(width // LANES):
        for j in range(blocks):
            line_ref[k, pl.ds(j, devices, stride=blocks)] = rows[
                k * devices : (k + 1) * devices, j * LANES : (j + 1) * LANES
            ]
    write_blocks(line_ref, outgoing_ref)


def expert_body(arrived_ref, gain_ref, gate_w, up_w, down_w, result_ref, x_ref, line_ref):
    tp_count = lax.axis_size("tp")
    ep_count = lax.axis_size("ep")
    devices, blocks, width = arrived_ref.shape
    own_width = blocks * LANES
    read_blocks(arrived_ref, line_ref)
    places = [
        (
            slice(k * ep_count, (k + 1) * ep_count),
            slice(part * own_width + j * LANES, part * own_width + (j + 1) * LANES),
            pl.ds(part * ep_count * blocks + j, ep_count, stride=blocks),
            k,
        )
        for k in range(width // LANES)
        for part in range(tp_count)
        for j in range(blocks)
    ]
    for row, column, line, k in places:
        x_ref[row, column] = line_ref[k, line]
    rows = x_ref[...]
    scale = lax.rsqrt(jnp.mean(rows * rows, axis=-1, keepdims=True) + norm_epsilon)
    ffn_in = (rows * scale * gain_ref[...]).astype(jnp.bfloat16)
    hidden = (silu(dot_bf16(ffn_in, gate_w[...])) * dot_bf16(ffn_in, up_w[...])).astype(jnp.bfloat16)
    result = dot_bf16(hidden, down_w[...])
    for row, column, line, k in places:
        line_ref[k, line] = result[row, column]
    write_blocks(line_ref, result_ref)


def combine_body(returned_ref, residual_ref, high_ref, low_ref, out_ref, line_ref):
    devices, blocks, width = returned_ref.shape
    read_blocks(returned_ref, line_ref)
    for j in range(blocks):
        rows = jnp.concatenate(
            [
                line_ref[k, pl.ds(j, devices, stride=blocks)]
                for k in range(width // LANES)
            ],
            axis=0,
        ).astype(jnp.bfloat16)
        moe_sum = dot_bf16(high_ref[...], rows) + dot_bf16(low_ref[...], rows)
        span = slice(j * LANES, (j + 1) * LANES)
        out_ref[:, span] = (residual_ref[:, span].astype(jnp.float32) + moe_sum).astype(jnp.bfloat16)


IN_VMEM = pl.BlockSpec(memory_space=pltpu.VMEM)
IN_HBM = pl.BlockSpec(memory_space=pltpu.HBM)


def resident(array):
    return pltpu.with_memory_space_constraint(array, pltpu.VMEM)


def grant(mebibytes):
    return pltpu.CompilerParams(vmem_limit_bytes=mebibytes * 2**20)


def local_fast(
    tokens,
    mix_gain,
    w_gate_z,
    w_value_x,
    w_key_b,
    w_query_c,
    w_step,
    step_bias,
    decay_log,
    skip_gain,
    conv_x_weight,
    conv_b_weight,
    conv_c_weight,
    window_x,
    window_b,
    window_c,
    ssm_state,
    head_gain,
    w_out,
    ffn_gain,
    route_ids,
    route_weights,
    expert_gate,
    expert_up,
    expert_down,
):
    tp_count = lax.axis_size("tp")
    ep_count = lax.axis_size("ep")
    seqs, own_width = tokens.shape
    model_width = w_gate_z.shape[0]
    width = w_gate_z.shape[1]
    devices = ep_count * tp_count
    bf16 = jnp.bfloat16
    f32 = jnp.float32
    capacity = capacity_of(seqs, route_ids.shape[1], devices)
    blocks = own_width // LANES
    lines = devices * capacity
    moved_shape = (devices, blocks, capacity * LANES)
    line_scratch = pltpu.VMEM((capacity, devices * blocks, LANES), f32)

    def shift(array, k):
        return lax.ppermute(array, "tp", [(i, i ^ k) for i in range(tp_count)])

    own = pl.pallas_call(
        entry_body,
        out_shape=pltpu.VMEM((seqs, own_width), bf16),
        in_specs=[IN_HBM],
        out_specs=IN_VMEM,
        scratch_shapes=[pltpu.SemaphoreType.DMA((seqs // ROW_TILE,))],
        compiler_params=grant(4),
        cost_estimate=pl.CostEstimate(flops=2 * 10**10, bytes_accessed=2**25, transcendentals=0),
        name="entry",
    )(pltpu.with_memory_space_constraint(tokens, pltpu.HBM))
    pieces = tuple(shift(own, k) for k in range(1, tp_count))
    chosen, high, low = pl.pallas_call(
        route_body,
        out_shape=(
            pltpu.VMEM((lines, seqs), bf16),
            pltpu.VMEM((seqs, lines), bf16),
            pltpu.VMEM((seqs, lines), bf16),
        ),
        in_specs=[IN_VMEM] * 2,
        out_specs=(IN_VMEM,) * 3,
        compiler_params=grant(4),
        cost_estimate=pl.CostEstimate(flops=10**10, bytes_accessed=2**24, transcendentals=0),
        name="route",
    )(route_ids.T, route_weights.T)
    (parts,) = pl.pallas_call(
        mixer_body,
        out_shape=(
            (pltpu.VMEM((seqs, own_width), f32),) + (pltpu.VMEM((seqs, own_width), bf16),) * (tp_count - 1),
        ),
        in_specs=[IN_VMEM, (IN_VMEM,) * (tp_count - 1)] + [IN_VMEM] * 18,
        out_specs=((IN_VMEM,) * tp_count,),
        scratch_shapes=[
            pltpu.VMEM((seqs, width), f32),
            pltpu.VMEM((seqs, model_width), bf16),
            pltpu.VMEM((seqs, STATE), f32),
        ],
        compiler_params=grant(4),
        name="mixer",
    )(
        own,
        pieces,
        mix_gain[None],
        w_step.T,
        step_bias[None],
        decay_log[None],
        skip_gain[None],
        conv_x_weight,
        conv_b_weight,
        conv_c_weight,
        jnp.swapaxes(window_x, 0, 1),
        jnp.swapaxes(window_b, 0, 1),
        jnp.swapaxes(window_c, 0, 1),
        head_gain[None],
        resident(w_gate_z),
        resident(w_value_x),
        resident(w_key_b),
        resident(w_query_c),
        resident(ssm_state.reshape(seqs, width, STATE)),
        resident(w_out),
    )
    shares = (parts[0],) + tuple(shift(parts[k], k) for k in range(1, tp_count))
    residual, outgoing = pl.pallas_call(
        pack_body,
        out_shape=(pltpu.VMEM((seqs, own_width), bf16), pltpu.VMEM(moved_shape, bf16)),
        in_specs=[IN_VMEM, (IN_VMEM,) * tp_count, IN_VMEM],
        out_specs=(IN_VMEM, IN_VMEM),
        scratch_shapes=[line_scratch],
        compiler_params=grant(4),
        name="pack",
    )(own, shares, chosen)

    def exchange(sent):
        return lax.all_to_all(sent, ("tp", "ep"), split_axis=0, concat_axis=0, tiled=True)

    result = pl.pallas_call(
        expert_body,
        out_shape=pltpu.VMEM(moved_shape, bf16),
        in_specs=[IN_VMEM] * 5,
        out_specs=IN_VMEM,
        scratch_shapes=[pltpu.VMEM((ep_count * capacity, model_width), f32), line_scratch],
        compiler_params=grant(4),
        name="expert",
    )(
        exchange(outgoing),
        ffn_gain[None],
        resident(expert_gate[0]),
        resident(expert_up[0]),
        resident(expert_down[0]),
    )
    return pl.pallas_call(
        combine_body,
        out_shape=jax.ShapeDtypeStruct((seqs, own_width), bf16),
        in_specs=[IN_VMEM] * 4,
        out_specs=IN_VMEM,
        scratch_shapes=[line_scratch],
        compiler_params=grant(4),
        name="combine",
    )(exchange(result), residual, high, low)


def capacity_of(seqs, top_count, experts):
    return max(2, (3 * seqs * top_count + 2 * experts - 1) // (2 * experts))


def local(*arrays):
    tokens, w_gate_z = arrays[0], arrays[2]
    seqs, own_width = tokens.shape
    width = w_gate_z.shape[1]
    tp_count = lax.axis_size("tp")
    fits = (
        tp_count == EXP_IN
        and lax.axis_size("ep") % ROW_TILE == 0
        and seqs % ROW_TILE == 0
        and own_width % LANES == 0
        and width % LANES == 0
    )
    return (local_fast if fits else local_generic)(*arrays)


def solution(mesh):
    in_specs = (
        P("ep", "tp"),
        P(),
        P(None, "tp"),
        P(None, "tp"),
        P(),
        P(),
        P(),
        P(),
        P(),
        P(),
        P(None, "tp"),
        P(),
        P(),
        P("ep", None, "tp"),
        P("ep", None, None),
        P("ep", None, None),
        P("ep", "tp", None, None),
        P("tp"),
        P("tp", None),
        P(),
        P("ep", None),
        P("ep", None),
        P("ep", None, "tp"),
        P("ep", None, "tp"),
        P("ep", "tp", None),
    )
    out_specs = P("ep", "tp")
    return jax.shard_map(local, mesh=mesh, in_specs=in_specs, out_specs=out_specs, check_vma=False)
```

```python
import jax
import jax.numpy as jnp
from jax import lax
from jax.experimental import pallas as pl
from jax.experimental.pallas import tpu as pltpu
from jax.sharding import PartitionSpec as P

HEADS = 32
HEAD_DIM = 64
STATE = 128
GROUPS = 2
EXP_IN = 4


norm_epsilon = 1e-06


def row_norm(arr_values, norm_gain):
    widened = arr_values.astype(jnp.float32)
    return (
        widened
        * lax.rsqrt(jnp.mean(widened * widened, axis=-1, keepdims=True) + norm_epsilon)
        * norm_gain
    )


def short_conv(window, fresh_row, weight):
    conv_taps = weight.astype(jnp.float32)
    summed = (
        jnp.sum(window.astype(jnp.float32) * conv_taps[:-1][None], axis=1)
        + fresh_row * conv_taps[-1]
    )
    return jax.nn.silu(summed)


def product(left, right):
    return jnp.dot(left, right, preferred_element_type=jnp.float32)


def local_generic(
    tokens,
    mix_gain,
    w_gate_z,
    w_value_x,
    w_key_b,
    w_query_c,
    w_step,
    step_bias,
    decay_log,
    skip_gain,
    conv_x_weight,
    conv_b_weight,
    conv_c_weight,
    window_x,
    window_b,
    window_c,
    ssm_state,
    head_gain,
    w_out,
    ffn_gain,
    route_ids,
    route_weights,
    expert_gate,
    expert_up,
    expert_down,
):
    tp_index = lax.axis_index("tp")
    tp_count = lax.axis_size("tp")
    ep_count = lax.axis_size("ep")
    seq_count = tokens.shape[0]
    gathered = lax.all_gather(tokens, "tp", axis=1, tiled=True)
    normed = row_norm(gathered, mix_gain).astype(jnp.bfloat16)
    local_width = w_gate_z.shape[1]
    head_count = local_width // HEAD_DIM
    first_head = tp_index * head_count
    group_start = first_head // (HEADS // GROUPS) * STATE
    gate_z = product(normed, w_gate_z)
    values = short_conv(window_x, product(normed, w_value_x), conv_x_weight)
    key_b = short_conv(
        lax.dynamic_slice_in_dim(window_b, group_start, STATE, 2),
        product(normed, lax.dynamic_slice_in_dim(w_key_b, group_start, STATE, 1)),
        lax.dynamic_slice_in_dim(conv_b_weight, group_start, STATE, 1),
    )
    query_c = short_conv(
        lax.dynamic_slice_in_dim(window_c, group_start, STATE, 2),
        product(normed, lax.dynamic_slice_in_dim(w_query_c, group_start, STATE, 1)),
        lax.dynamic_slice_in_dim(conv_c_weight, group_start, STATE, 1),
    )
    step_all = product(normed, w_step) + step_bias
    step_size = jax.nn.softplus(lax.dynamic_slice_in_dim(step_all, first_head, head_count, 1))
    rate_heads = jnp.exp(lax.dynamic_slice_in_dim(decay_log, first_head, head_count, 0))
    skip_heads = lax.dynamic_slice_in_dim(skip_gain, first_head, head_count, 0)
    decay_heads = jnp.exp(-step_size * rate_heads)
    value_heads = values.reshape(seq_count, head_count, HEAD_DIM)
    new_state = (
        decay_heads[:, :, None, None] * ssm_state
        + (step_size[:, :, None] * value_heads)[..., None] * key_b[:, None, None, :]
    )
    read_out = jnp.einsum("shpn,sn->shp", new_state, query_c, precision=lax.Precision.HIGHEST)
    read_out = read_out + skip_heads[None, :, None] * value_heads
    gated = read_out * jax.nn.silu(gate_z.reshape(seq_count, head_count, HEAD_DIM))
    gated = gated * lax.rsqrt(jnp.mean(gated * gated, axis=-1, keepdims=True) + norm_epsilon)
    mixed_heads = (
        (gated * head_gain.reshape(head_count, HEAD_DIM))
        .reshape(seq_count, local_width)
        .astype(jnp.bfloat16)
    )
    partial_value = product(mixed_heads, w_out)
    share_mix = lax.psum_scatter(partial_value, "tp", scatter_dimension=1, tiled=True)
    residual_own = (tokens.astype(jnp.float32) + share_mix).astype(jnp.bfloat16)
    residual_full = lax.all_gather(residual_own, "tp", axis=1, tiled=True)
    ffn_in = row_norm(residual_full, ffn_gain).astype(jnp.bfloat16)
    top_count = route_ids.shape[1]
    expert_count = EXP_IN * ep_count
    capacity = max(2, (3 * seq_count * top_count + 2 * expert_count - 1) // (2 * expert_count))
    sub_index = tp_index // (tp_count // EXP_IN)
    target_set = route_ids // EXP_IN
    hit_mask = route_ids % EXP_IN == sub_index
    set_grid = jnp.arange(ep_count, dtype=jnp.int32)
    set_onehot = (hit_mask[:, :, None] & (target_set[:, :, None] == set_grid)).astype(jnp.int32)
    set_onehot = set_onehot.reshape(seq_count * top_count, ep_count)
    earlier = jnp.cumsum(set_onehot, axis=0) - set_onehot
    slot_rank = jnp.sum(earlier * set_onehot, axis=1).reshape(seq_count, top_count)
    slot_index = jnp.where(hit_mask, target_set * capacity + slot_rank, -1)
    slot_grid = jnp.arange(ep_count * capacity, dtype=jnp.int32)
    slot_match = slot_index[:, :, None] == slot_grid
    placed = jnp.any(slot_match, axis=1).astype(jnp.bfloat16)
    outgoing = jnp.einsum("sj,sd->jd", placed, ffn_in, preferred_element_type=jnp.float32)
    outgoing = outgoing.astype(jnp.bfloat16).reshape(ep_count, capacity, ffn_in.shape[1])
    route_share = route_weights / jnp.sum(route_weights, axis=1, keepdims=True)
    combine_weight = jnp.sum(jnp.where(slot_match, route_share[:, :, None], 0.0), axis=1)
    arrived = lax.all_to_all(outgoing, "ep", split_axis=0, concat_axis=0, tiled=True)
    source_count, slot_count, row_width = arrived.shape
    flat_rows = arrived.reshape(source_count * slot_count, row_width)
    gate_part = product(flat_rows, expert_gate[0])
    up_part = product(flat_rows, expert_up[0])
    hidden = (jax.nn.silu(gate_part) * up_part).astype(jnp.bfloat16)
    expert_out = product(hidden, expert_down[0]).reshape(source_count, slot_count, row_width)
    returned = lax.all_to_all(
        expert_out.astype(jnp.bfloat16), "ep", split_axis=0, concat_axis=0, tiled=True
    ).astype(expert_out.dtype)
    moe_part = jnp.dot(
        combine_weight,
        returned.reshape(ep_count * capacity, -1),
        precision=lax.Precision.HIGHEST,
        preferred_element_type=jnp.float32,
    )
    moe_share = lax.psum_scatter(
        moe_part.astype(jnp.bfloat16), "tp", scatter_dimension=1, tiled=True
    ).astype(jnp.float32)
    return (residual_own.astype(jnp.float32) + moe_share).astype(jnp.bfloat16)


ROW_TILE = 8
LANES = 128
VECTOR_SEQS = 16


def dot_bf16(left, right):
    return lax.dot_general(left, right, (((1,), (0,)), ((), ())), preferred_element_type=jnp.float32)


def dot_nt(left, right):
    return lax.dot_general(left, right, (((1,), (1,)), ((), ())), preferred_element_type=jnp.float32)


def halves(array):
    high = array.astype(jnp.bfloat16)
    return high, (array - high.astype(jnp.float32)).astype(jnp.bfloat16)


def silu(value):
    return value / (1.0 + jnp.exp(-value))


def conv_rows(window_ref, columns, fresh, taps_ref):
    taps = taps_ref[:, columns].astype(jnp.float32)
    count = window_ref.shape[0]
    summed = fresh * taps[count : count + 1]
    for tap in range(count):
        summed = summed + window_ref[tap, :, columns].astype(jnp.float32) * taps[tap : tap + 1]
    return silu(summed)


def mixer_body(
    own_ref,
    piece_refs,
    gain_ref,
    step_w_ref,
    bias_ref,
    rate_ref,
    skip_ref,
    tap_x_ref,
    tap_b_ref,
    tap_c_ref,
    win_x_ref,
    win_b_ref,
    win_c_ref,
    head_gain_ref,
    gate_w,
    value_w,
    key_w,
    query_w,
    state,
    out_w,
    part_refs,
    y_ref,
    row_ref,
    query_ref,
):
    tp_index = lax.axis_index("tp")
    seqs, width = y_ref.shape
    head_count = width // HEAD_DIM
    first_head = tp_index * head_count
    group = first_head // (HEADS // GROUPS)
    columns = pl.ds(pl.multiple_of(group * STATE, STATE), STATE)
    blocks = seqs // ROW_TILE
    own_width = own_ref.shape[1]
    for k, piece_ref in enumerate((own_ref, *piece_refs)):
        row_ref[:, pl.ds(pl.multiple_of((tp_index ^ k) * own_width, own_width), own_width)] = piece_ref[...]
    rows = row_ref[...].astype(jnp.float32)
    scale = lax.rsqrt(jnp.mean(rows * rows, axis=-1, keepdims=True) + norm_epsilon)
    normed = (rows * scale * gain_ref[...]).astype(jnp.bfloat16)
    step_size = jax.nn.softplus(dot_nt(normed, step_w_ref[...]) + bias_ref[...])
    decay = jnp.exp(-step_size * jnp.exp(rate_ref[...]))
    key_row = dot_bf16(normed, key_w[:, columns])
    query_row = dot_bf16(normed, query_w[:, columns])
    value_row = dot_bf16(normed, value_w[...])
    gate_z = dot_bf16(normed, gate_w[...])
    keys = conv_rows(win_b_ref, columns, key_row, tap_b_ref)
    queries = conv_rows(win_c_ref, columns, query_row, tap_c_ref)
    overlap = jnp.sum(keys * queries, axis=-1, keepdims=True)
    query_hi, query_lo = halves(queries)
    row_of = lax.broadcasted_iota(jnp.int32, (ROW_TILE, width), 0)
    lane = lax.broadcasted_iota(jnp.int32, (LANES, LANES), 1)
    query_ref[...] = queries
    first_block = VECTOR_SEQS // ROW_TILE
    for b in range(max(blocks - first_block, width // LANES)):
        if b < width // LANES:
            span = slice(b * LANES, (b + 1) * LANES)
            turned = jnp.zeros((LANES, LANES), jnp.float32)
            for i in range(VECTOR_SEQS):
                summed = jnp.sum(state[i, span] * query_ref[i : i + 1], axis=-1, keepdims=True)
                turned = jnp.where(lane == i, summed, turned)
            y_ref[:VECTOR_SEQS, span] = turned.T[:VECTOR_SEQS]
        if first_block + b < blocks:
            start = (first_block + b) * ROW_TILE
            lines = slice(start, start + ROW_TILE)
            both = jnp.concatenate([query_hi[lines], query_lo[lines]], axis=0)
            total = jnp.zeros((ROW_TILE, width), jnp.float32)
            for i in range(ROW_TILE):
                found = dot_nt(both, state[start + i].astype(jnp.bfloat16))
                total = jnp.where(row_of == i, found[:ROW_TILE] + found[ROW_TILE:], total)
            y_ref[lines] = total
    spread = (
        lax.broadcasted_iota(jnp.int32, (2 * HEADS, width), 0) % HEADS
        == first_head + lax.broadcasted_iota(jnp.int32, (2 * HEADS, width), 1) // HEAD_DIM
    ).astype(jnp.bfloat16)
    per_head = jnp.concatenate(
        [decay, step_size, jnp.broadcast_to(skip_ref[...], (ROW_TILE, HEADS))], axis=0
    )
    wide = dot_bf16(jnp.concatenate(halves(per_head), axis=1), spread)
    values = conv_rows(win_x_ref, slice(None), value_row, tap_x_ref)
    read_out = wide[:seqs] * y_ref[...] + (wide[seqs : 2 * seqs] * overlap + wide[2 * seqs : 2 * seqs + 1]) * values
    gated = read_out * silu(gate_z)
    same_head = (
        lax.broadcasted_iota(jnp.int32, (LANES, LANES), 0) // HEAD_DIM
        == lax.broadcasted_iota(jnp.int32, (LANES, LANES), 1) // HEAD_DIM
    ).astype(jnp.bfloat16)
    scaled = []
    for j in range(0, width, LANES):
        block = gated[:, j : j + LANES]
        sums = dot_bf16(jnp.concatenate(halves(block * block), axis=0), same_head)
        mean_sq = (sums[:seqs] + sums[seqs:]) * (1.0 / HEAD_DIM)
        scaled.append(block * lax.rsqrt(mean_sq + norm_epsilon) * head_gain_ref[:, j : j + LANES])
    mixed = jnp.concatenate(scaled, axis=1).astype(jnp.bfloat16)
    for k, part_ref in enumerate(part_refs):
        span = pl.ds(pl.multiple_of((tp_index ^ k) * own_width, own_width), own_width)
        part_ref[...] = dot_bf16(mixed, out_w[:, span]).astype(part_ref.dtype)


def slots_of(ids_ref, experts, lines):
    seqs = ids_ref.shape[1]
    line = lax.broadcasted_iota(jnp.int32, (lines, seqs), 0)
    sets = lax.axis_size("ep")
    expert = line % sets * EXP_IN + line % experts // sets
    first = ids_ref[0:1, :] == expert
    second = ids_ref[1:2, :] == expert
    hit = jnp.logical_or(first, second)
    before = (
        lax.broadcasted_iota(jnp.int32, (seqs, seqs), 0) < lax.broadcasted_iota(jnp.int32, (seqs, seqs), 1)
    ).astype(jnp.bfloat16)
    rank = dot_bf16(hit.astype(jnp.bfloat16), before)
    place = (line // experts).astype(jnp.float32)
    return jnp.logical_and(hit, rank == place), first


def entry_body(own_hbm, own_ref, sems):
    copies = []
    for i in range(sems.shape[0]):
        span = pl.ds(i * ROW_TILE, ROW_TILE)
        copies.append(pltpu.make_async_copy(own_hbm.at[span], own_ref.at[span], sems.at[i]))
    for copy in copies:
        copy.start()
    for copy in copies:
        copy.wait()


def route_body(ids_ref, weight_ref, chosen_ref, high_ref, low_ref):
    experts = EXP_IN * lax.axis_size("ep")
    chosen, first = slots_of(ids_ref, experts, chosen_ref.shape[0])
    chosen_ref[...] = chosen.astype(jnp.bfloat16)
    weights = weight_ref[...]
    share = weights / jnp.sum(weights, axis=0, keepdims=True)
    picked = jnp.where(chosen, jnp.where(first, share[0:1, :], share[1:2, :]), 0.0).T
    high_ref[...], low_ref[...] = halves(picked)


def write_blocks(line_ref, moved_ref):
    devices, blocks, width = moved_ref.shape
    for d in range(devices):
        for k in range(width // LANES):
            moved_ref[d, :, k * LANES : (k + 1) * LANES] = line_ref[
                k, d * blocks : (d + 1) * blocks
            ].astype(moved_ref.dtype)


def read_blocks(moved_ref, line_ref):
    devices, blocks, width = moved_ref.shape
    for d in range(devices):
        for k in range(width // LANES):
            line_ref[k, d * blocks : (d + 1) * blocks] = moved_ref[
                d, :, k * LANES : (k + 1) * LANES
            ].astype(line_ref.dtype)


def pack_body(own_ref, part_refs, chosen_ref, residual_ref, outgoing_ref, line_ref):
    share = own_ref[...].astype(jnp.float32)
    for part_ref in part_refs:
        share = share + part_ref[...].astype(jnp.float32)
    residual = share.astype(jnp.bfloat16)
    residual_ref[...] = residual
    rows = dot_bf16(chosen_ref[...], residual)
    devices, blocks, width = outgoing_ref.shape
    for k in range(width // LANES):
        for j in range(blocks):
            line_ref[k, pl.ds(j, devices, stride=blocks)] = rows[
                k * devices : (k + 1) * devices, j * LANES : (j + 1) * LANES
            ]
    write_blocks(line_ref, outgoing_ref)


def expert_body(arrived_ref, gain_ref, gate_w, up_w, down_w, result_ref, x_ref, line_ref):
    tp_count = lax.axis_size("tp")
    ep_count = lax.axis_size("ep")
    devices, blocks, width = arrived_ref.shape
    own_width = blocks * LANES
    read_blocks(arrived_ref, line_ref)
    places = [
        (
            slice(k * ep_count, (k + 1) * ep_count),
            slice(part * own_width + j * LANES, part * own_width + (j + 1) * LANES),
            pl.ds(part * ep_count * blocks + j, ep_count, stride=blocks),
            k,
        )
        for k in range(width // LANES)
        for part in range(tp_count)
        for j in range(blocks)
    ]
    for row, column, line, k in places:
        x_ref[row, column] = line_ref[k, line]
    rows = x_ref[...]
    scale = lax.rsqrt(jnp.mean(rows * rows, axis=-1, keepdims=True) + norm_epsilon)
    raised = (rows * gain_ref[...]).astype(jnp.bfloat16)
    gate_part = dot_bf16(raised, gate_w[...]) * scale
    hidden = (silu(gate_part) * (dot_bf16(raised, up_w[...]) * scale)).astype(jnp.bfloat16)
    result = dot_bf16(hidden, down_w[...])
    for row, column, line, k in places:
        line_ref[k, line] = result[row, column]
    write_blocks(line_ref, result_ref)


def combine_body(returned_ref, residual_ref, high_ref, low_ref, out_ref, line_ref):
    devices, blocks, width = returned_ref.shape
    read_blocks(returned_ref, line_ref)
    for j in range(blocks):
        rows = jnp.concatenate(
            [
                line_ref[k, pl.ds(j, devices, stride=blocks)]
                for k in range(width // LANES)
            ],
            axis=0,
        ).astype(jnp.bfloat16)
        moe_sum = dot_bf16(high_ref[...], rows) + dot_bf16(low_ref[...], rows)
        span = slice(j * LANES, (j + 1) * LANES)
        out_ref[:, span] = (residual_ref[:, span].astype(jnp.float32) + moe_sum).astype(jnp.bfloat16)


IN_VMEM = pl.BlockSpec(memory_space=pltpu.VMEM)
IN_HBM = pl.BlockSpec(memory_space=pltpu.HBM)


def resident(array):
    return pltpu.with_memory_space_constraint(array, pltpu.VMEM)


def grant(mebibytes):
    return pltpu.CompilerParams(vmem_limit_bytes=mebibytes * 2**20)


def local_fast(
    tokens,
    mix_gain,
    w_gate_z,
    w_value_x,
    w_key_b,
    w_query_c,
    w_step,
    step_bias,
    decay_log,
    skip_gain,
    conv_x_weight,
    conv_b_weight,
    conv_c_weight,
    window_x,
    window_b,
    window_c,
    ssm_state,
    head_gain,
    w_out,
    ffn_gain,
    route_ids,
    route_weights,
    expert_gate,
    expert_up,
    expert_down,
):
    tp_count = lax.axis_size("tp")
    ep_count = lax.axis_size("ep")
    seqs, own_width = tokens.shape
    model_width = w_gate_z.shape[0]
    width = w_gate_z.shape[1]
    devices = ep_count * tp_count
    bf16 = jnp.bfloat16
    f32 = jnp.float32
    capacity = capacity_of(seqs, route_ids.shape[1], devices)
    blocks = own_width // LANES
    lines = devices * capacity
    moved_shape = (devices, blocks, capacity * LANES)
    line_scratch = pltpu.VMEM((capacity, devices * blocks, LANES), f32)

    def shift(array, k):
        return lax.ppermute(array, "tp", [(i, i ^ k) for i in range(tp_count)])

    own = pl.pallas_call(
        entry_body,
        out_shape=pltpu.VMEM((seqs, own_width), bf16),
        in_specs=[IN_HBM],
        out_specs=IN_VMEM,
        scratch_shapes=[pltpu.SemaphoreType.DMA((seqs // ROW_TILE,))],
        compiler_params=grant(4),
        cost_estimate=pl.CostEstimate(flops=2 * 10**10, bytes_accessed=2**25, transcendentals=0),
        name="entry",
    )(pltpu.with_memory_space_constraint(tokens, pltpu.HBM))
    pieces = tuple(shift(own, k) for k in range(1, tp_count))
    chosen, high, low = pl.pallas_call(
        route_body,
        out_shape=(
            pltpu.VMEM((lines, seqs), bf16),
            pltpu.VMEM((seqs, lines), bf16),
            pltpu.VMEM((seqs, lines), bf16),
        ),
        in_specs=[IN_VMEM] * 2,
        out_specs=(IN_VMEM,) * 3,
        compiler_params=grant(4),
        cost_estimate=pl.CostEstimate(flops=10**10, bytes_accessed=2**24, transcendentals=0),
        name="route",
    )(route_ids.T, route_weights.T)
    (parts,) = pl.pallas_call(
        mixer_body,
        out_shape=(
            (pltpu.VMEM((seqs, own_width), f32),) + (pltpu.VMEM((seqs, own_width), bf16),) * (tp_count - 1),
        ),
        in_specs=[IN_VMEM, (IN_VMEM,) * (tp_count - 1)] + [IN_VMEM] * 18,
        out_specs=((IN_VMEM,) * tp_count,),
        scratch_shapes=[
            pltpu.VMEM((seqs, width), f32),
            pltpu.VMEM((seqs, model_width), bf16),
            pltpu.VMEM((seqs, STATE), f32),
        ],
        compiler_params=grant(4),
        name="mixer",
    )(
        own,
        pieces,
        mix_gain[None],
        w_step.T,
        step_bias[None],
        decay_log[None],
        skip_gain[None],
        conv_x_weight,
        conv_b_weight,
        conv_c_weight,
        jnp.swapaxes(window_x, 0, 1),
        jnp.swapaxes(window_b, 0, 1),
        jnp.swapaxes(window_c, 0, 1),
        head_gain[None],
        resident(w_gate_z),
        resident(w_value_x),
        resident(w_key_b),
        resident(w_query_c),
        resident(ssm_state.reshape(seqs, width, STATE)),
        resident(w_out),
    )
    shares = (parts[0],) + tuple(shift(parts[k], k) for k in range(1, tp_count))
    residual, outgoing = pl.pallas_call(
        pack_body,
        out_shape=(pltpu.VMEM((seqs, own_width), bf16), pltpu.VMEM(moved_shape, bf16)),
        in_specs=[IN_VMEM, (IN_VMEM,) * tp_count, IN_VMEM],
        out_specs=(IN_VMEM, IN_VMEM),
        scratch_shapes=[line_scratch],
        compiler_params=grant(4),
        name="pack",
    )(own, shares, chosen)

    def exchange(sent):
        return lax.all_to_all(sent, ("tp", "ep"), split_axis=0, concat_axis=0, tiled=True)

    result = pl.pallas_call(
        expert_body,
        out_shape=pltpu.VMEM(moved_shape, bf16),
        in_specs=[IN_VMEM] * 5,
        out_specs=IN_VMEM,
        scratch_shapes=[pltpu.VMEM((ep_count * capacity, model_width), f32), line_scratch],
        compiler_params=grant(4),
        name="expert",
    )(
        exchange(outgoing),
        ffn_gain[None],
        resident(expert_gate[0]),
        resident(expert_up[0]),
        resident(expert_down[0]),
    )
    return pl.pallas_call(
        combine_body,
        out_shape=jax.ShapeDtypeStruct((seqs, own_width), bf16),
        in_specs=[IN_VMEM] * 4,
        out_specs=IN_VMEM,
        scratch_shapes=[line_scratch],
        compiler_params=grant(4),
        name="combine",
    )(exchange(result), residual, high, low)


def capacity_of(seqs, top_count, experts):
    return max(2, (3 * seqs * top_count + 2 * experts - 1) // (2 * experts))


def local(*arrays):
    tokens, w_gate_z = arrays[0], arrays[2]
    seqs, own_width = tokens.shape
    width = w_gate_z.shape[1]
    tp_count = lax.axis_size("tp")
    fits = (
        tp_count == EXP_IN
        and lax.axis_size("ep") % ROW_TILE == 0
        and seqs % ROW_TILE == 0
        and own_width % LANES == 0
        and width % LANES == 0
    )
    return (local_fast if fits else local_generic)(*arrays)


def solution(mesh):
    in_specs = (
        P("ep", "tp"),
        P(),
        P(None, "tp"),
        P(None, "tp"),
        P(),
        P(),
        P(),
        P(),
        P(),
        P(),
        P(None, "tp"),
        P(),
        P(),
        P("ep", None, "tp"),
        P("ep", None, None),
        P("ep", None, None),
        P("ep", "tp", None, None),
        P("tp"),
        P("tp", None),
        P(),
        P("ep", None),
        P("ep", None),
        P("ep", None, "tp"),
        P("ep", None, "tp"),
        P("ep", "tp", None),
    )
    out_specs = P("ep", "tp")
    return jax.shard_map(local, mesh=mesh, in_specs=in_specs, out_specs=out_specs, check_vma=False)
```
